32 devices in a mesh: fs: 16 (over z, y, x), tp: 2 (over core).
Axes of the slice: x: 2, y: 2, z: 4, core: 2. Of those that a mesh axis runs over, the one named last changes fastest.
Arguments:
- tokens: bfloat16 [4096, 2048], P('fs'), may hold values from -6 to 6
- routes: int32 [4096, 6], P('fs'), may hold values from 0 to 15, all different within a row; in each aligned block of 256 rows (0 to 255, 256 to 511, ...) at most 160 rows name the same one
- route_weights: float32 [4096, 6], P('fs'), may hold values from 0.1 to 1
- norm_gain: float32 [2048], P('fs'), may hold values from 0.1 to 1.9
- expert_gate: float32 [16, 2048, 1024], P(None, 'fs', 'tp'), may hold values from -0.125 to 0.125
- expert_up: float32 [16, 2048, 1024], P(None, 'fs', 'tp'), may hold values from -0.125 to 0.125
- expert_down: float32 [16, 2048, 1024], P(None, 'fs', 'tp'), may hold values from -0.1875 to 0.1875
- shared_gate: float32 [2048, 1024], P('fs', 'tp'), may hold values from -0.125 to 0.125
- shared_up: float32 [2048, 1024], P('fs', 'tp'), may hold values from -0.125 to 0.125
- shared_down: float32 [2048, 1024], P('fs', 'tp'), may hold values from -0.1875 to 0.1875
Outputs:
- layer_output: bfloat16 [4096, 2048], P('fs', 'tp')
- sample_gate: bfloat16 [16, 2048, 1024], P('fs', None, 'tp')
- sample_up: bfloat16 [16, 2048, 1024], P('fs', None, 'tp')
- sample_down: bfloat16 [16, 2048, 1024], P('fs', None, 'tp')
- common_gate: bfloat16 [2048, 1024], P(None, 'tp')
- common_up: bfloat16 [2048, 1024], P(None, 'tp')
- common_down: bfloat16 [2048, 1024], P(None, 'tp')
The draws below stay inside these ranges and needn't reach their ends.
Inputs may be any that keep to these rules, and one draw needn't show every extreme that they name: `routes`: each row names 6 different experts. In each aligned block of 256 rows (the rows of one index of fs) no expert is named by more than 160 rows, a bound that some expert reaches in some blocks.
All inputs are finite; a program needn't handle non-finite values.
Results may differ from the reference program's by a relative error of at most 0.015.
Values may be sent and summed in bfloat16 or wider, within the bound.
A program may use at most 128 MiB of HBM per device.

```python
import math
import jax
import jax.numpy as jnp
import numpy as np
from jax import lax

D = 2048
FF = 1024
SH = 1024
TOP = 6
TOK_DEV = 256
EXPERTS = 16
CAP = 160
TOKENS = 4096
N_FS = 16
N_TP = 2


def block_scale(stream_key, dims, split, least, high):
    gain = 1.0
    for dim, blocks in split:
        draws = jax.random.uniform(jax.random.fold_in(jax.random.fold_in(stream_key, 6), dim), (blocks,), jnp.float32, least / len(split), high / len(split))
        gain = gain * jnp.repeat(jnp.exp(draws), dims[dim] // blocks).reshape((-1,) + (1,) * (len(dims) - 1 - dim))
    return gain


def deal_out(key, own, number, rows, count, top, bound, slope):
    ranking = jax.random.permutation(key, count)
    heavy_load, ordinary = shares(count, rows * top, bound, slope, True), shares(count, rows * top, bound, slope, False)
    places = jnp.arange(count)

    def named(tallies, rotation):
        used = int((tallies > 0).sum())
        fixed = max(1, used // 4)
        shifted = fixed + (places - fixed + rotation * (used - fixed)) % max(1, count - fixed)
        return jnp.zeros((count,), jnp.int32).at[ranking[jnp.where(places < fixed, places, shifted)]].set(jnp.asarray(tallies, jnp.int32))

    tallies = jnp.where(number % 4 == 0, named(heavy_load, number // 4), named(ordinary, number - number // 4 - 1))
    mixed = jax.random.permutation(jax.random.fold_in(own, 3), count)
    giver, taker = mixed[0:count // 2 * 2:2], mixed[1:count // 2 * 2:2]
    room = jnp.minimum(tallies[giver] - 1, bound - tallies[taker]) // 2
    room = jnp.where((giver == ranking[0]) | (taker == ranking[0]) | (tallies[taker] == 0), 0, jnp.maximum(room, 0))
    shifted = jax.random.randint(jax.random.fold_in(own, 4), (count // 2,), 0, 1 << 20) % (room + 1)
    tallies = tallies.at[giver].add(-shifted).at[taker].add(shifted)
    items = jnp.searchsorted(jnp.cumsum(tallies), jnp.arange(rows * top), side="right").astype(jnp.int32)
    table = items.reshape(top, rows).T
    table = table[jax.random.permutation(jax.random.fold_in(own, 1), rows)]
    rotation = jax.random.randint(jax.random.fold_in(own, 2), (rows, 1), 0, top)
    return jnp.take_along_axis(table, (jnp.arange(top)[None, :] + rotation) % top, axis=1)


def shares(number_of, total, limit, slope, full):
    portions = [(1 << 20) // math.isqrt(grade ** slope) + 1 for grade in range(1, number_of + 1)]
    largest = limit if full else min(limit, max(-(-total // number_of), total * portions[0] // sum(portions)))
    least = 1 if total - largest >= number_of - 1 else 0
    counts, rest = [largest] + [least] * (number_of - 1), total - largest - least * (number_of - 1)
    while rest > 0:
        free = [i for i in range(1, number_of) if counts[i] < largest] or [i for i in range(1, number_of) if counts[i] < limit]
        pool, budget = sum([portions[i] for i in free]), rest
        for i in free:
            extra = min(limit - counts[i], max(1, budget * portions[i] // pool), rest)
            counts[i] = counts[i] + extra
            rest = rest - extra
    return np.array(counts)


def normal_values(stream_key, shape, scale, limit, shards=(), kind=jnp.bfloat16):
    result = scale * jax.random.normal(stream_key, shape, jnp.float32)
    if shards:
        result = result * block_scale(stream_key, shape, shards, -0.22, 0.18)
    return jnp.clip(result, -limit, limit).astype(kind)


def setup_inputs(seed: int = 0) -> dict:
    streams_of = jax.random.split(jax.random.key(seed), 11)
    tokens = normal_values(streams_of[0], (TOKENS, D), 1.0, 6.0, ((0, 16),))
    routes_keys = jax.random.split(jax.random.fold_in(streams_of[1], 1), TOKENS // TOK_DEV)
    routes_turns = jax.random.permutation(jax.random.fold_in(streams_of[1], 3), TOKENS // TOK_DEV)
    routes = jax.vmap(lambda own, number: deal_out(jax.random.fold_in(streams_of[1], 2), own, number, TOK_DEV, EXPERTS, TOP, CAP, 1))(routes_keys, routes_turns).reshape((TOKENS, TOP))
    route_weights = jnp.clip(jnp.exp(math.log(1.0) - 2.3025851 * jax.random.uniform(streams_of[2], (TOKENS, TOP), jnp.float32) ** block_scale(streams_of[2], (TOKENS, TOP), ((0, 16),), -0.2, 0.2)), 0.1, 1.0)
    norm_gain = jnp.clip(1.0 + 0.18 * jax.random.normal(streams_of[3], (D,), jnp.float32), 0.1, 1.9)
    expert_gate = normal_values(streams_of[4], (EXPERTS, D, FF), D ** -0.5, 0.125, ((1, 16), (2, 2)), jnp.float32)
    expert_up = normal_values(streams_of[5], (EXPERTS, D, FF), D ** -0.5, 0.125, ((1, 16), (2, 2)), jnp.float32)
    expert_down = normal_values(streams_of[6], (EXPERTS, D, FF), FF ** -0.5, 0.1875, ((1, 16), (2, 2)), jnp.float32)
    shared_gate = normal_values(streams_of[7], (D, SH), D ** -0.5, 0.125, ((0, 16), (1, 2)), jnp.float32)
    shared_up = normal_values(streams_of[8], (D, SH), D ** -0.5, 0.125, ((0, 16), (1, 2)), jnp.float32)
    shared_down = normal_values(streams_of[9], (D, SH), SH ** -0.5, 0.1875, ((0, 16), (1, 2)), jnp.float32)
    return dict(tokens=tokens, routes=routes, route_weights=route_weights, norm_gain=norm_gain, expert_gate=expert_gate, expert_up=expert_up, expert_down=expert_down, shared_gate=shared_gate, shared_up=shared_up, shared_down=shared_down)


EPSILON = 1e-06

def normalize(tokens):
    values = tokens.astype(jnp.float32)
    scale = lax.rsqrt(lax.optimization_barrier(jnp.mean(values * values, axis=-1, keepdims=True)) + EPSILON)
    return (values * scale).astype(jnp.bfloat16)

def block_sum(hidden, down):
    block_width = hidden.shape[1] // N_TP
    total = jnp.zeros((hidden.shape[0], down.shape[0]), jnp.float32)
    for block in range(N_TP):
        lower = block * block_width
        part = jnp.dot(hidden[:, lower:lower + block_width], down[:, lower:lower + block_width].T, preferred_element_type=jnp.float32).astype(jnp.bfloat16)
        part = lax.optimization_barrier(part)
        total = total + part.astype(jnp.float32)
    return total

def reference(tokens, routes, route_weights, norm_gain, expert_gate, expert_up, expert_down, shared_gate, shared_up, shared_down):
    sample_gate = (norm_gain[None, :, None] * expert_gate).astype(jnp.bfloat16)
    sample_up = (norm_gain[None, :, None] * expert_up).astype(jnp.bfloat16)
    sample_down = expert_down.astype(jnp.bfloat16)
    common_gate = (norm_gain[:, None] * shared_gate).astype(jnp.bfloat16)
    common_up = (norm_gain[:, None] * shared_up).astype(jnp.bfloat16)
    common_down = shared_down.astype(jnp.bfloat16)
    normed = normalize(tokens)
    route_blocks = routes.reshape(N_FS, TOK_DEV * TOP)
    member = (route_blocks[:, :, None] == jnp.arange(EXPERTS, dtype=jnp.int32)[None, None, :]).astype(jnp.int32)
    before = lax.optimization_barrier(jnp.sum((jnp.cumsum(member, axis=1) - member) * member, axis=2))
    block_index = jnp.arange(N_FS, dtype=jnp.int32)[:, None]
    slots = (route_blocks * (N_FS * CAP) + block_index * CAP + before).reshape(-1)
    row_index = (block_index * TOK_DEV + jnp.arange(TOK_DEV * TOP, dtype=jnp.int32)[None, :] // TOP).reshape(-1)
    sources = jnp.full((EXPERTS * N_FS * CAP,), TOKENS, jnp.int32).at[slots].set(row_index)
    padded = jnp.concatenate([normed, jnp.zeros((1, D), jnp.bfloat16)], axis=0)

    def per_expert(operands):
        expert_rows, gate_w, up_w, down_w = operands
        rows = padded[expert_rows]
        gate = jnp.dot(rows, gate_w, preferred_element_type=jnp.float32)
        upward = jnp.dot(rows, up_w, preferred_element_type=jnp.float32)
        hidden = (jax.nn.silu(gate) * upward).astype(jnp.bfloat16)
        return block_sum(hidden, down_w).astype(jnp.bfloat16)
    expert_out = lax.map(per_expert, (sources.reshape(EXPERTS, N_FS * CAP), sample_gate, sample_up, sample_down))
    picked = expert_out.reshape(EXPERTS * N_FS * CAP, D)[slots].astype(jnp.float32).reshape(TOKENS, TOP, D)
    routed = lax.optimization_barrier(jnp.sum(picked * route_weights[:, :, None], axis=1))
    shared_gate_act = jnp.dot(normed, common_gate, preferred_element_type=jnp.float32)
    shared_up_act = jnp.dot(normed, common_up, preferred_element_type=jnp.float32)
    shared_hidden = (jax.nn.silu(shared_gate_act) * shared_up_act).astype(jnp.bfloat16)
    shared_sum = block_sum(shared_hidden, common_down)
    layer_output = (routed + shared_sum).astype(jnp.bfloat16)
    return (layer_output, sample_gate, sample_up, sample_down, common_gate, common_up, common_down)
```

```python
import functools

import jax
import jax.numpy as jnp
from jax import lax
from jax.experimental import pallas as pl
from jax.experimental.pallas import tpu as pltpu
from jax.sharding import PartitionSpec as P

MESH = pl.DeviceIdType.MESH
EPSILON = 1e-06


def normalize(tokens):
    values = tokens.astype(jnp.float32)
    scale = lax.rsqrt(jnp.mean(values * values, axis=-1, keepdims=True) + EPSILON)
    return (values * scale).astype(jnp.bfloat16)


def place():
    fs = lax.axis_index("fs")
    return fs, lax.axis_index("tp"), fs % 2, (fs // 2) % 2, fs // 4


def barrier_all(fs, tp):
    count = lax.axis_size("fs")
    sem = pltpu.get_barrier_semaphore()
    for step in range(1, count):
        pl.semaphore_signal(
            sem, inc=1, device_id=((fs + step) % count, tp), device_id_type=MESH
        )
    pl.semaphore_signal(sem, inc=1, device_id=(fs, 1 - tp), device_id_type=MESH)
    pl.semaphore_wait(sem, count)


def partner_at(step, x, y, z, sign):
    offset = (7 * step) % 16
    dz, dy, dx = offset // 4, (offset // 2) % 2, offset % 2
    return ((z + 4 + sign * dz) % 4) * 4 + ((y + dy) % 2) * 2 + (x + dx) % 2


def gather_kernel(
    tensors, tok_ref, scale_ref, gain_ref, *refs
):
    raw = refs[:tensors]
    tok_all, scale_all = refs[tensors : tensors + 2]
    own = refs[tensors + 2 : 2 * tensors + 2]
    other = refs[2 * tensors + 2 : 3 * tensors + 2]
    (
        tok_own, wide, narrow,
        load_sem, tok_send, tok_recv, fwd_send, sc_send, sc_recv,
        w_send, w_recv, p_send, p_recv, loc_sem,
    ) = refs[3 * tensors + 2 :]
    fs, tp, x, y, z = place()
    plane = fs % 4
    xp, yp = fs + 1 - 2 * x, fs + 2 - 4 * y
    rows = raw[0].shape[1]
    share = tok_own.shape[0]

    def remote(src, dst, ssem, rsem, to, core=None):
        return pltpu.make_async_remote_copy(
            src_ref=src, dst_ref=dst, send_sem=ssem, recv_sem=rsem,
            device_id=(to, tp if core is None else core), device_id_type=MESH,
        )

    def load(t, to):
        return pltpu.make_async_copy(raw[t].at[to], wide.at[t, to], load_sem.at[t, to])

    def start_loads(step, _):
        for t in range(tensors):
            load(t, partner_at(step, x, y, z, 1)).start()
        return _

    lax.fori_loop(1, 17, start_loads, 0)
    tok_own[...] = normalize(tok_ref[...])
    gain = gain_ref[...]

    def convert(step, _):
        to = partner_at(step, x, y, z, 1)
        for t in range(tensors):
            load(t, to).wait()
            block = wide[t, to]
            narrow[t, to] = (block * gain if t < 2 else block).astype(jnp.bfloat16)
        return _

    def weight(t, to):
        return remote(
            narrow.at[t, to], own[t].at[pl.ds(fs * rows, rows)],
            w_send.at[t, to], w_recv.at[t, fs], to,
        )

    def send(step, _):
        to = partner_at(step, x, y, z, 1)
        for t in range(tensors):
            weight(t, to).start()
        return _

    def slot(pl_index, block):
        return pl_index * 4 + block

    def tok_copy(pl_index, block, sem, to, src=None):
        s = slot(pl_index, block)
        return remote(
            tok_all.at[s] if src is None else src, tok_all.at[s], sem, tok_recv.at[s], to
        )

    def line_copies(block, src=None):
        return (
            (z < 3, block <= z, tok_copy(plane, block, tok_send.at[0, block], fs + 4, src)),
            (z > 0, block >= z, tok_copy(plane, block, tok_send.at[1, block], fs - 4, src)),
            (None, None, tok_copy(plane, block, tok_send.at[2, block], xp, src)),
            (None, None, tok_copy(plane, block, tok_send.at[3, block], yp, src)),
        )

    def spread(block, src=None):
        for room, side, copy in line_copies(block, src):
            if room is None:
                copy.start()
            else:
                pl.when(jnp.logical_and(room, side))(copy.start)

    def arrive(block):
        s = slot(plane, block)
        remote(tok_all.at[s], tok_all.at[s], tok_send.at[0, block], tok_recv.at[s], fs + 4).wait_recv()
        spread(block)

    xplane, yplane = plane + 1 - 2 * x, plane + 2 - 4 * y

    def fwd_copy(block, low):
        s = slot(xplane if low else yplane, block)
        return remote(
            tok_all.at[s], tok_all.at[s], fwd_send.at[block], tok_recv.at[s], yp if low else xp
        )

    def plane_forward(block):
        @pl.when(jnp.logical_and(block >= 0, block < 2))
        def _():
            copy = fwd_copy(block, True)
            copy.wait_recv()
            copy.start()

        @pl.when(jnp.logical_and(block >= 2, block < 4))
        def _():
            copy = fwd_copy(block, False)
            copy.wait_recv()
            copy.start()

    batch = 3
    lax.fori_loop(1, 1 + batch, convert, 0)
    barrier_all(fs, tp)

    spread(z, tok_own)
    own_tok = pltpu.make_async_copy(tok_own, tok_all.at[slot(plane, z)], loc_sem.at[0])
    own_tok.start()

    def scale_copy(step):
        to = (fs + step) % 16
        return remote(
            scale_ref.at[to], scale_all.at[slot(plane, z)], sc_send.at[to],
            sc_recv.at[slot(plane, z)], to,
        )

    own_scale = pltpu.make_async_copy(scale_ref.at[fs], scale_all.at[slot(plane, z)], loc_sem.at[1])
    own_scale.start()

    def send_scale(step, _):
        scale_copy(step).start()
        return _

    lax.fori_loop(1, 16, send_scale, 0)

    for stage in range(5):
        lax.fori_loop(1 + batch * stage, 1 + batch * (stage + 1), send, 0)
        lax.fori_loop(
            1 + batch * (stage + 1), min(17, 1 + batch * (stage + 2)), convert, 0
        )
        if stage < 3:
            pl.when(z - stage - 1 >= 0)(lambda: arrive(z - stage - 1))
            pl.when(z + stage + 1 < 4)(lambda: arrive(z + stage + 1))
        if stage == 0:
            plane_forward(z)
        elif stage < 4:
            plane_forward(z - stage)
            plane_forward(z + stage)

    def local(t):
        return pltpu.make_async_copy(
            narrow.at[t, fs], own[t].at[pl.ds(fs * rows, rows)], loc_sem.at[2 + t]
        )

    def across(t, frm, src):
        return remote(
            src, other[t].at[pl.ds(frm * rows, rows)], p_send.at[t, frm], p_recv.at[t, frm],
            fs, 1 - tp,
        )

    for t in range(tensors):
        local(t).start()
        across(t, fs, narrow.at[t, fs]).start()

    def pass_on(step, _):
        frm = partner_at(step, x, y, z, -1)
        for t in range(tensors):
            piece = own[t].at[pl.ds(frm * rows, rows)]
            remote(piece, piece, w_send.at[t, frm], w_recv.at[t, frm], frm).wait_recv()
            across(t, frm, piece).start()
        return _

    lax.fori_loop(1, 16, pass_on, 0)

    own_tok.wait()
    own_scale.wait()
    for t in range(tensors):
        local(t).wait()

    def drain_send(step, _):
        to = partner_at(step, x, y, z, 1)
        for t in range(tensors):
            weight(t, to).wait_send()
        scale_copy(step).wait_send()
        return _

    lax.fori_loop(1, 16, drain_send, 0)

    def drain_across(step, _):
        for t in range(tensors):
            across(t, step, own[t].at[pl.ds(step * rows, rows)]).wait()
        return _

    lax.fori_loop(0, 16, drain_across, 0)

    for block in range(4):
        for room, side, copy in line_copies(block):
            if room is None:
                copy.wait_send()
            else:
                pl.when(jnp.logical_and(room, side))(copy.wait_send)
        fwd_copy(block, block < 2).wait_send()

        def landed(pl_index):
            s = slot(pl_index, block)
            remote(tok_all.at[s], tok_all.at[s], tok_send.at[0, 0], tok_recv.at[s], xp).wait_recv()

        landed(yplane if block < 2 else xplane)
        landed(3 - plane)

    def drain_scale(step, _):
        other_fs = (fs + step) % 16
        s = slot(other_fs % 4, other_fs // 4)
        remote(
            scale_all.at[s], scale_all.at[s], sc_send.at[0], sc_recv.at[s], other_fs
        ).wait_recv()
        return _

    lax.fori_loop(1, 16, drain_scale, 0)


def gather(tokens_share, dense, gain, raws, cid):
    experts, rows, half = raws[0].shape
    share, width = tokens_share.shape
    n = len(raws)
    hbm, vmem = pl.BlockSpec(memory_space=pl.ANY), pl.BlockSpec(memory_space=pltpu.VMEM)
    weight = jax.ShapeDtypeStruct((experts * rows, half), jnp.bfloat16)
    dma = pltpu.SemaphoreType.DMA
    return pl.pallas_call(
        functools.partial(gather_kernel, n),
        out_shape=[
            jax.ShapeDtypeStruct((16, share, width), jnp.bfloat16),
            jax.ShapeDtypeStruct((16, 1, share), jnp.float32),
        ] + [weight] * (2 * n),
        in_specs=[vmem, vmem, vmem] + [hbm] * n,
        out_specs=[hbm, vmem] + [hbm] * (2 * n),
        scratch_shapes=[
            pltpu.VMEM((share, width), jnp.bfloat16),
            pltpu.VMEM((n, experts, rows, half), jnp.float32),
            pltpu.VMEM((n, experts, rows, half), jnp.bfloat16),
            dma((n, 16)), dma((4, 4)), dma((16,)), dma((4,)), dma((16,)), dma((16,)),
            dma((n, 16)), dma((n, 16)), dma((n, 16)), dma((n, 16)), dma((2 + n,)),
        ],
        compiler_params=pltpu.CompilerParams(
            collective_id=cid, has_side_effects=True, vmem_limit_bytes=48 << 20
        ),
    )(tokens_share, dense, gain, *raws)


def ring_of(fs_count):
    if fs_count != 16:
        return list(range(fs_count))
    order = []
    for place, column in enumerate((0, 1, 3, 2)):
        heights = range(4) if place % 2 == 0 else range(3, -1, -1)
        order.extend(height * 4 + column for height in heights)
    return order


def reorder(blocks, order):
    if list(order) == list(range(len(order))):
        return blocks
    return jnp.concatenate([blocks[i : i + 1] for i in order], axis=0)


def general_body(
    tokens,
    routes,
    route_weights,
    norm_gain,
    expert_gate,
    expert_up,
    expert_down,
    shared_gate,
    shared_up,
    shared_down,
):
    tp_count = lax.axis_size("tp")
    tp_index = lax.axis_index("tp")
    fs_count = lax.axis_size("fs")
    tok_rows, width = tokens.shape
    experts = expert_gate.shape[0]
    share = tok_rows // tp_count
    own_experts = experts // fs_count
    ring = ring_of(fs_count)
    place_of = [ring.index(i) for i in range(fs_count)]
    groups = None if ring == list(range(fs_count)) else [ring]

    normed = normalize(tokens)
    own_normed = lax.dynamic_slice_in_dim(normed, tp_index * share, share, 0)
    own_routes = lax.dynamic_slice_in_dim(routes, tp_index * share, share, 0)
    own_weights = lax.dynamic_slice_in_dim(route_weights, tp_index * share, share, 0)
    member = own_routes[None, :, :] == jnp.arange(experts, dtype=jnp.int32)[:, None, None]
    dense = jnp.sum(jnp.where(member, own_weights[None, :, :], 0.0), axis=2)
    dense_all = lax.all_gather(dense, "fs", axis=0, tiled=False)
    own_normed, dense_all = lax.optimization_barrier((own_normed, dense_all))
    gathered = lax.all_gather(own_normed, "fs", axis=0, tiled=False)
    gathered = reorder(gathered, ring).reshape(fs_count * share, width)

    gain_rows = norm_gain[None, :, None]
    rounded = (
        (expert_gate * gain_rows).astype(jnp.bfloat16),
        (expert_up * gain_rows).astype(jnp.bfloat16),
        expert_down.astype(jnp.bfloat16),
    )
    sample_gate, sample_up, sample_down = (
        lax.all_to_all(rounded[0], "fs", split_axis=0, concat_axis=1, tiled=True),
        lax.all_to_all(rounded[1], "fs", split_axis=0, concat_axis=1, tiled=True),
        lax.all_to_all(rounded[2], "fs", split_axis=0, concat_axis=1, tiled=True),
    )

    half = shared_gate.shape[1]
    shared_rows = jnp.concatenate(
        [
            (shared_gate * norm_gain[:, None]).astype(jnp.bfloat16),
            (shared_up * norm_gain[:, None]).astype(jnp.bfloat16),
            shared_down.astype(jnp.bfloat16),
        ],
        axis=1,
    )
    common = lax.all_gather(shared_rows, "fs", axis=0, tiled=False, axis_index_groups=groups)
    common_gate, common_up, common_down = (
        reorder(common[:, :, i * half : (i + 1) * half], place_of).reshape(width, half)
        for i in range(3)
    )
    shared_gate_act = jnp.dot(normed, common_gate, preferred_element_type=jnp.float32)
    shared_up_act = jnp.dot(normed, common_up, preferred_element_type=jnp.float32)
    shared_hidden = (jax.nn.silu(shared_gate_act) * shared_up_act).astype(jnp.bfloat16)
    shared_part = jnp.einsum(
        "th,dh->td", shared_hidden, common_down, preferred_element_type=jnp.float32
    ).astype(jnp.bfloat16)
    shared_parts = lax.all_to_all(
        shared_part.reshape(tok_rows, tp_count, width // tp_count).transpose(1, 0, 2),
        "tp",
        split_axis=0,
        concat_axis=0,
        tiled=True,
    )
    shared_sum = jnp.sum(shared_parts.astype(jnp.float32), axis=0)

    scale_all = reorder(
        lax.dynamic_slice_in_dim(
            dense_all, lax.axis_index("fs") * own_experts, own_experts, 1
        ),
        ring,
    )
    total = None
    for expert in range(own_experts):
        scale = scale_all[:, expert, :].reshape(-1)[:, None]
        for shift in range(tp_count):
            gate_w, up_w, down_w = (
                sample_gate[expert],
                sample_up[expert],
                sample_down[expert],
            )
            if shift:
                pairs = [(i, (i + shift) % tp_count) for i in range(tp_count)]
                gate_w, up_w, down_w = (
                    lax.ppermute(gate_w, "tp", pairs),
                    lax.ppermute(up_w, "tp", pairs),
                    lax.ppermute(down_w, "tp", pairs),
                )
            gate = jnp.dot(gathered, gate_w, preferred_element_type=jnp.float32)
            upward = jnp.dot(gathered, up_w, preferred_element_type=jnp.float32)
            hidden = (jax.nn.silu(gate) * upward * scale).astype(jnp.bfloat16)
            part = jnp.einsum("rf,df->rd", hidden, down_w, preferred_element_type=jnp.float32)
            total = part if total is None else total + part
    routed = lax.psum_scatter(
        total.astype(jnp.bfloat16), "fs", scatter_dimension=0, tiled=True, axis_index_groups=groups
    )
    routed = lax.all_to_all(routed, "tp", split_axis=1, concat_axis=0, tiled=True)
    layer_output = (routed.astype(jnp.float32) + shared_sum).astype(jnp.bfloat16)
    return (layer_output, sample_gate, sample_up, sample_down, common_gate, common_up, common_down)


def block_body(
    tokens, routes, route_weights, norm_gain,
    expert_gate, expert_up, expert_down,
    shared_gate, shared_up, shared_down,
):
    tp_index = lax.axis_index("tp")
    tok_rows, width = tokens.shape
    experts = expert_gate.shape[0]
    share = tok_rows // 2
    own_routes = lax.dynamic_slice_in_dim(routes, tp_index * share, share, 0)
    own_weights = lax.dynamic_slice_in_dim(route_weights, tp_index * share, share, 0)
    own_tokens = lax.dynamic_slice_in_dim(tokens, tp_index * share, share, 0)
    member = own_routes[None, :, :] == jnp.arange(experts, dtype=jnp.int32)[:, None, None]
    dense = jnp.sum(jnp.where(member, own_weights[None, :, :], 0.0), axis=2)
    gathered, scale, sample_gate, sample_up, sample_down, gate_o, up_o, down_o = gather(
        own_tokens, dense[:, None, :], norm_gain[:, None],
        (expert_gate, expert_up, expert_down), 1,
    )
    gathered = gathered.reshape(16 * share, width)
    scale = scale.reshape(16 * share, 1)
    normed = normalize(tokens)
    half = shared_gate.shape[1]
    shared_rows = jnp.concatenate(
        [
            (shared_gate * norm_gain[:, None]).astype(jnp.bfloat16),
            (shared_up * norm_gain[:, None]).astype(jnp.bfloat16),
            shared_down.astype(jnp.bfloat16),
        ],
        axis=1,
    )
    common = lax.all_gather(shared_rows, "fs", axis=0, tiled=True)
    common_gate, common_up, common_down = (
        common[:, i * half : (i + 1) * half] for i in range(3)
    )
    shared_hidden = (
        jax.nn.silu(jnp.dot(normed, common_gate, preferred_element_type=jnp.float32))
        * jnp.dot(normed, common_up, preferred_element_type=jnp.float32)
    ).astype(jnp.bfloat16)
    shared_part = jnp.einsum(
        "th,dh->td", shared_hidden, common_down, preferred_element_type=jnp.float32
    ).astype(jnp.bfloat16)
    shared_parts = lax.all_to_all(
        shared_part.reshape(tok_rows, 2, width // 2).transpose(1, 0, 2),
        "tp", split_axis=0, concat_axis=0, tiled=True,
    )
    shared_sum = jnp.sum(shared_parts.astype(jnp.float32), axis=0)
    total = None
    for gate_w, up_w, down_w in ((sample_gate, sample_up, sample_down), (gate_o, up_o, down_o)):
        gate = jnp.dot(gathered, gate_w, preferred_element_type=jnp.float32)
        upward = jnp.dot(gathered, up_w, preferred_element_type=jnp.float32)
        hidden = (jax.nn.silu(gate) * upward * scale).astype(jnp.bfloat16)
        part = jnp.einsum("rf,df->rd", hidden, down_w, preferred_element_type=jnp.float32)
        total = part if total is None else total + part
    order = [[plane + 4 * z for plane in range(4) for z in range(4)]]
    routed = lax.psum_scatter(
        total.astype(jnp.bfloat16), "fs", scatter_dimension=0, tiled=True, axis_index_groups=order
    )
    routed = lax.all_to_all(routed, "tp", split_axis=1, concat_axis=0, tiled=True)
    layer_output = (routed.astype(jnp.float32) + shared_sum).astype(jnp.bfloat16)
    return (
        layer_output, sample_gate[None], sample_up[None], sample_down[None],
        common_gate, common_up, common_down,
    )


def solution(mesh):
    fits = mesh.shape["fs"] == 16 and mesh.shape["tp"] == 2
    body = block_body if fits else general_body
    return jax.shard_map(
        body,
        mesh=mesh,
        in_specs=(
            P("fs", None),
            P("fs", None),
            P("fs", None),
            P("fs"),
            P(None, "fs", "tp"),
            P(None, "fs", "tp"),
            P(None, "fs", "tp"),
            P("fs", "tp"),
            P("fs", "tp"),
            P("fs", "tp"),
        ),
        out_specs=(
            P("fs", "tp"),
            P("fs", None, "tp"),
            P("fs", None, "tp"),
            P("fs", None, "tp"),
            P(None, "tp"),
            P(None, "tp"),
            P(None, "tp"),
        ),
        check_vma=False,
    )
```

```python
import functools

import jax
import jax.numpy as jnp
from jax import lax
from jax.experimental import pallas as pl
from jax.experimental.pallas import tpu as pltpu
from jax.sharding import PartitionSpec as P

MESH = pl.DeviceIdType.MESH
EPSILON = 1e-06
UNITS = (0, 3, 1, 2)


def normalize(tokens):
    values = tokens.astype(jnp.float32)
    scale = lax.rsqrt(jnp.mean(values * values, axis=-1, keepdims=True) + EPSILON)
    return (values * scale).astype(jnp.bfloat16)


def place():
    fs = lax.axis_index("fs")
    return fs, lax.axis_index("tp"), fs % 2, (fs // 2) % 2, fs // 4


def barrier_all(fs, tp):
    count = lax.axis_size("fs")
    sem = pltpu.get_barrier_semaphore()
    for step in range(1, count):
        pl.semaphore_signal(
            sem, inc=1, device_id=((fs + step) % count, tp), device_id_type=MESH
        )
    pl.semaphore_signal(sem, inc=1, device_id=(fs, 1 - tp), device_id_type=MESH)
    pl.semaphore_wait(sem, count)


def partner_at(step, x, y, z, sign):
    offset = (7 * step) % 16
    dz, dy, dx = offset // 4, (offset // 2) % 2, offset % 2
    return ((z + 4 + sign * dz) % 4) * 4 + ((y + dy) % 2) * 2 + (x + dx) % 2


def remote(src, dst, ssem, rsem, to, core):
    return pltpu.make_async_remote_copy(
        src_ref=src, dst_ref=dst, send_sem=ssem, recv_sem=rsem,
        device_id=(to, core), device_id_type=MESH,
    )


class Chain:
    def __init__(self, at, send_sem, fwd_sem, recv_sem):
        self.fs, self.tp, self.x, self.y, self.z = place()
        self.at, self.send_sem, self.fwd_sem, self.recv_sem = at, send_sem, fwd_sem, recv_sem
        self.plane = self.fs % 4
        self.xp, self.yp = self.fs + 1 - 2 * self.x, self.fs + 2 - 4 * self.y
        self.xplane, self.yplane = self.plane + 1 - 2 * self.x, self.plane + 2 - 4 * self.y

    def copy(self, slot, sem, to, src=None):
        here = self.at(slot)
        return remote(
            here if src is None else src, here, sem, self.recv_sem.at[slot], to, self.tp
        )

    def line(self, block, src=None):
        slot, z = block * 4 + self.plane, self.z
        return (
            (jnp.logical_and(z < 3, block <= z), self.copy(slot, self.send_sem.at[0, block], self.fs + 4, src)),
            (jnp.logical_and(z > 0, block >= z), self.copy(slot, self.send_sem.at[1, block], self.fs - 4, src)),
            (None, self.copy(slot, self.send_sem.at[2, block], self.xp, src)),
            (None, self.copy(slot, self.send_sem.at[3, block], self.yp, src)),
        )

    def spread(self, block, src=None):
        for cond, copy in self.line(block, src):
            if cond is None:
                copy.start()
            else:
                pl.when(cond)(copy.start)

    def landed(self, slot):
        self.copy(slot, self.send_sem.at[0, 0], self.xp).wait_recv()

    def arrive(self, block):
        self.landed(block * 4 + self.plane)
        self.spread(block)

    def forward_copy(self, block, low):
        slot = block * 4 + (self.xplane if low else self.yplane)
        return self.copy(slot, self.fwd_sem.at[block], self.yp if low else self.xp)

    def plane_forward(self, block):
        for low in (True, False):
            inside = (
                jnp.logical_and(block >= 0, block < 2)
                if low
                else jnp.logical_and(block >= 2, block < 4)
            )

            @pl.when(inside)
            def _(low=low):
                copy = self.forward_copy(block, low)
                copy.wait_recv()
                copy.start()

    def stage(self, step):
        z = self.z
        if step < 3:
            pl.when(z - step - 1 >= 0)(lambda: self.arrive(z - step - 1))
            pl.when(z + step + 1 < 4)(lambda: self.arrive(z + step + 1))
        if step == 0:
            self.plane_forward(z)
        elif step < 4:
            self.plane_forward(z - step)
            self.plane_forward(z + step)

    def finish(self):
        for block in range(4):
            self.landed(block * 4 + (self.yplane if block < 2 else self.xplane))
            self.landed(block * 4 + 3 - self.plane)

    def drain(self):
        for block in range(4):
            for cond, copy in self.line(block):
                if cond is None:
                    copy.wait_send()
                else:
                    pl.when(cond)(copy.wait_send)
            self.forward_copy(block, block < 2).wait_send()


class Exchange:
    def __init__(self, raw, wide, narrow, own, other, gain, sems):
        self.raw, self.wide, self.narrow, self.own, self.other = raw, wide, narrow, own, other
        self.gain = gain
        self.load_sem, self.send_sem, self.recv_sem, self.psend, self.precv = sems
        self.fs, self.tp, self.x, self.y, self.z = place()
        self.rows = raw[0].shape[1]
        self.count = len(raw)

    def partner(self, step, sign=1):
        return partner_at(step, self.x, self.y, self.z, sign)

    def load(self, t, to):
        return pltpu.make_async_copy(
            self.raw[t].at[to], self.wide.at[t, to], self.load_sem.at[t, to]
        )

    def each(self, lower, upper, body):
        def step(i, carry):
            for t in range(self.count):
                body(i, t)
            return carry

        lax.fori_loop(lower, upper, step, 0)

    def start_loads(self):
        self.each(1, 17, lambda i, t: self.load(t, self.partner(i)).start())

    def convert(self, lower, upper):
        def one(i, t):
            to = self.partner(i)
            self.load(t, to).wait()
            block = self.wide[t, to]
            if self.gain is not None:
                block = block * self.gain
            self.narrow[t, to] = block.astype(jnp.bfloat16)

        self.each(lower, upper, one)

    def piece(self, ref, frm):
        return ref.at[pl.ds(frm * self.rows, self.rows)]

    def copy(self, t, to):
        return remote(
            self.narrow.at[t, to], self.piece(self.own[t], self.fs),
            self.send_sem.at[t, to], self.recv_sem.at[t, self.fs], to, self.tp,
        )

    def send(self, lower, upper):
        self.each(lower, upper, lambda i, t: self.copy(t, self.partner(i)).start())

    def across(self, t, frm, src):
        return remote(
            src, self.piece(self.other[t], frm), self.psend.at[t, frm], self.precv.at[t, frm],
            self.fs, 1 - self.tp,
        )

    def pass_on(self):
        def one(i, t):
            frm = self.partner(i, -1)
            piece = self.piece(self.own[t], frm)
            remote(
                piece, piece, self.send_sem.at[t, frm], self.recv_sem.at[t, frm], frm, self.tp
            ).wait_recv()
            self.across(t, frm, piece).start()

        self.each(1, 16, one)

    def finish(self):
        self.each(
            0, 16, lambda i, t: self.across(t, i, self.piece(self.own[t], i)).wait()
        )

    def drain(self):
        self.each(1, 16, lambda i, t: self.copy(t, self.partner(i)).wait_send())


def gather_kernel(
    tok_ref, scale_ref, gain_ref, gate_ref, up_ref,
    tok_all, scale_all, gate_own, up_own, gate_other, up_other,
    tok_own, wide, narrow,
    chain_send, chain_fwd, chain_recv, sc_send, sc_recv,
    load_sem, w_send, w_recv, p_send, p_recv, loc_sem,
):
    fs, tp, x, y, z = place()
    ex = Exchange(
        (gate_ref, up_ref), wide, narrow, (gate_own, up_own), (gate_other, up_other),
        gain_ref[...], (load_sem, w_send, w_recv, p_send, p_recv),
    )
    chain = Chain(lambda slot: tok_all.at[slot], chain_send, chain_fwd, chain_recv)
    ex.start_loads()
    tok_own[...] = normalize(tok_ref[...])
    batch = 3
    ex.convert(1, 1 + batch)
    barrier_all(fs, tp)
    chain.spread(z, tok_own)
    own_tok = pltpu.make_async_copy(tok_own, tok_all.at[fs], loc_sem.at[0])
    own_tok.start()
    own_scale = pltpu.make_async_copy(scale_ref.at[fs], scale_all.at[fs], loc_sem.at[1])
    own_scale.start()

    def scale_copy(to):
        return remote(
            scale_ref.at[to], scale_all.at[fs], sc_send.at[to], sc_recv.at[fs], to, tp
        )

    def send_scale(step, carry):
        scale_copy((fs + step) % 16).start()
        return carry

    lax.fori_loop(1, 16, send_scale, 0)
    for stage in range(5):
        ex.send(1 + batch * stage, 1 + batch * (stage + 1))
        ex.convert(1 + batch * (stage + 1), min(17, 1 + batch * (stage + 2)))
        chain.stage(stage)

    def local(t):
        return pltpu.make_async_copy(narrow.at[t, fs], ex.piece(ex.own[t], fs), loc_sem.at[2 + t])

    for t in range(2):
        local(t).start()
        ex.across(t, fs, narrow.at[t, fs]).start()
    ex.pass_on()
    own_tok.wait()
    own_scale.wait()
    for t in range(2):
        local(t).wait()
    chain.finish()
    ex.finish()
    chain.drain()
    ex.drain()

    def drain_scale(step, carry):
        frm = (fs + step) % 16
        scale_copy(frm).wait_send()
        here = scale_all.at[frm]
        remote(here, here, sc_send.at[frm], sc_recv.at[frm], frm, tp).wait_recv()
        return carry

    lax.fori_loop(1, 16, drain_scale, 0)


def dot_nt(a, b):
    return lax.dot_general(a, b, (((1,), (1,)), ((), ())), preferred_element_type=jnp.float32)


def mix_kernel(
    tok_ref, scale_ref, gain_ref, sgate_ref, sup_ref, sdown_ref,
    tok_all, gate_own, up_own, gate_other, up_other, down_ref,
    out_ref, sample_down, common_gate, common_up, common_down,
    acts, gate_up, down_v, wide, narrow, hidden, common, normed,
    shid, spart, spart_in, fin, fin_in, xd_in, yd_in, xg_in, yg_in, zb_in, za_in,
    chain_send, chain_fwd, chain_recv, load_sem, w_send, w_recv, p_send, p_recv,
    d_send, d_recv, g_send, g_recv, z_send, z_recv, e_send, e_recv, loc_sem,
):
    fs, tp, x, y, z = place()
    ex = Exchange(
        (down_ref,), wide, narrow, (down_v.at[0],), (down_v.at[1],), None,
        (load_sem, w_send, w_recv, p_send, p_recv),
    )
    rows, half = sgate_ref.shape
    width = tok_ref.shape[1]
    chain = Chain(
        lambda slot: common.at[pl.ds(slot * rows, rows)], chain_send, chain_fwd, chain_recv
    )
    share = acts.shape[1] // 4

    ex.start_loads()
    loads = [
        pltpu.make_async_copy(src, gate_up.at[t, h], loc_sem.at[2 * t + h])
        for t, pair in enumerate(((gate_own, gate_other), (up_own, up_other)))
        for h, src in enumerate(pair)
    ] + [
        pltpu.make_async_copy(
            tok_all.at[pl.ds(b * 4 * share, 4 * share)], acts.at[b], loc_sem.at[4 + b]
        )
        for b in UNITS
    ]
    for copy in loads:
        copy.start()
    gain = gain_ref[...]
    mine = pl.ds(fs * rows, rows)
    common[mine, 0:half] = (sgate_ref[...] * gain).astype(jnp.bfloat16)
    common[mine, half : 2 * half] = (sup_ref[...] * gain).astype(jnp.bfloat16)
    common[mine, 2 * half : 3 * half] = sdown_ref[...].astype(jnp.bfloat16)
    batch = 3
    ex.convert(1, 1 + batch)
    barrier_all(fs, tp)
    chain.spread(z)
    ex.send(1, 1 + batch)
    ex.convert(1 + batch, 17)
    normed[...] = normalize(tok_ref[...])
    for copy in loads:
        copy.wait()

    tile = 256
    per_half = half // tile

    def gate_up_unit(b):
        def step(j, carry):
            h, c = j // per_half, j % per_half
            cols = pl.ds(pl.multiple_of(c * tile, tile), tile)
            a = acts[b]
            gate = jnp.dot(a, gate_up[0, h, :, cols], preferred_element_type=jnp.float32)
            up = jnp.dot(a, gate_up[1, h, :, cols], preferred_element_type=jnp.float32)
            scale = scale_ref[pl.ds(b * 4 * share, 4 * share), :]
            hidden[b, :, pl.ds(pl.multiple_of(j * tile, tile), tile)] = (
                jax.nn.silu(gate) * up * scale
            ).astype(jnp.bfloat16)
            return carry

        lax.fori_loop(0, 2 * per_half, step, 0)

    for index, b in enumerate(UNITS):
        gate_up_unit(b)
        chain.stage(index)
        ex.send(1 + batch * (index + 1), 1 + batch * (index + 2))

    own_down = pltpu.make_async_copy(narrow.at[0, fs], ex.piece(sample_down, fs), loc_sem.at[0])
    own_down.start()
    down_v[0, mine, :] = narrow[0, fs]
    ex.across(0, fs, narrow.at[0, fs]).start()
    ex.pass_on()
    ex.finish()

    def put_down(i, carry):
        frm = ex.partner(i)
        pltpu.make_async_copy(
            ex.piece(down_v.at[0], frm), ex.piece(sample_down, frm), load_sem.at[0, frm]
        ).start()
        return carry

    lax.fori_loop(1, 16, put_down, 0)

    plane = fs % 4
    xp, yp = chain.xp, chain.yp
    xplane, yplane, dplane = chain.xplane, chain.yplane, 3 - plane
    mid = width // 2
    lo, hi = pl.ds(0, mid), pl.ds(mid, mid)

    def part(b, which, cols):
        return acts.at[b, pl.ds(which * share, share), cols]

    def down_unit(b):
        def step(n, carry):
            cols = pl.ds(pl.multiple_of(n * tile, tile), tile)
            acts[b, :, cols] = (
                dot_nt(hidden[b, :, 0:half], down_v[0, cols, :])
                + dot_nt(hidden[b, :, half : 2 * half], down_v[1, cols, :])
            ).astype(jnp.bfloat16)
            return carry

        lax.fori_loop(0, width // tile, step, 0)

    def d_copies(b):
        return (
            remote(part(b, dplane, lo), xd_in.at[b], d_send.at[0, b], d_recv.at[0, b], xp, tp),
            remote(part(b, dplane, hi), yd_in.at[b], d_send.at[1, b], d_recv.at[1, b], yp, tp),
        )

    def g_copy(b, kind):
        which, cols, box, to = (
            (xplane, lo, xg_in, xp),
            (xplane, hi, xg_in, xp),
            (yplane, hi, yg_in, yp),
            (yplane, lo, yg_in, yp),
        )[kind]
        return remote(
            part(b, which, cols), box.at[b, :, cols], g_send.at[kind, b], g_recv.at[kind, b],
            to, tp,
        )

    def first(b):
        for copy in d_copies(b):
            copy.start()
        g_copy(b, 0).start()
        g_copy(b, 2).start()

    def add_into(ref, others):
        total = ref[...].astype(jnp.float32)
        for other in others:
            total = total + other[...].astype(jnp.float32)
        ref[...] = total.astype(jnp.bfloat16)

    def combine(b):
        x_copy, y_copy = d_copies(b)
        x_copy.wait_recv()
        add_into(part(b, yplane, lo), [xd_in.at[b]])
        g_copy(b, 3).start()
        y_copy.wait_recv()
        add_into(part(b, xplane, hi), [yd_in.at[b]])
        g_copy(b, 1).start()

    every = pl.ds(0, width)

    def z_copy(b, way):
        box = (zb_in, za_in)[way]
        return remote(
            part(b, plane, every), box.at[b], z_send.at[way, b], z_recv.at[way, b],
            fs + (4, -4)[way], tp,
        )

    def settle(b):
        for kind in range(4):
            g_copy(b, kind).wait_recv()
        add_into(part(b, plane, every), [xg_in.at[b], yg_in.at[b]])
        if b > 0:
            pl.when(z == 0)(z_copy(b, 0).start)
        if b < 3:
            pl.when(z == 3)(z_copy(b, 1).start)

    def relay(b):
        if b > 0:
            @pl.when(jnp.logical_and(z > 0, z < b))
            def _():
                z_copy(b, 0).wait_recv()
                add_into(part(b, plane, every), [zb_in.at[b]])
                z_copy(b, 0).start()

        if b < 3:
            @pl.when(jnp.logical_and(z < 3, z > b))
            def _():
                z_copy(b, 1).wait_recv()
                add_into(part(b, plane, every), [za_in.at[b]])
                z_copy(b, 1).start()

    def finish(b):
        @pl.when(z == b)
        def _():
            boxes = []
            if b > 0:
                z_copy(b, 0).wait_recv()
                boxes.append(zb_in)
            if b < 3:
                z_copy(b, 1).wait_recv()
                boxes.append(za_in)
            for side in range(2):
                cols = pl.ds(side * mid, mid)
                total = acts[b, pl.ds(plane * share, share), cols].astype(jnp.float32)
                for box in boxes:
                    total = total + box[b, :, cols].astype(jnp.float32)
                fin[side] = total.astype(jnp.bfloat16)

    u0, u1, u2, u3 = UNITS
    down_unit(u0)
    first(u0)
    chain.stage(4)
    down_unit(u1)
    first(u1)
    combine(u0)
    down_unit(u2)
    first(u2)
    combine(u1)
    down_unit(u3)
    first(u3)

    chain.finish()
    puts = [
        pltpu.make_async_copy(
            common.at[:, pl.ds(i * half, half)], ref, loc_sem.at[1 + i]
        )
        for i, ref in enumerate((common_gate, common_up, common_down))
    ]
    for copy in puts:
        copy.start()

    def shared_step(c, carry):
        a = normed[...]
        cols = pl.ds(pl.multiple_of(c * tile, tile), tile)
        gate = jnp.dot(a, common[:, cols], preferred_element_type=jnp.float32)
        up = jnp.dot(
            a, common[:, pl.ds(pl.multiple_of(half + c * tile, tile), tile)],
            preferred_element_type=jnp.float32,
        )
        shid[:, cols] = (jax.nn.silu(gate) * up).astype(jnp.bfloat16)
        return carry

    def shared_down_step(n, carry):
        per = mid // tile
        spart[n // per, :, pl.ds(pl.multiple_of((n % per) * tile, tile), tile)] = dot_nt(
            shid[...],
            common[pl.ds(pl.multiple_of(n * tile, tile), tile), 2 * half : 3 * half],
        ).astype(jnp.bfloat16)
        return carry

    lax.fori_loop(0, per_half, shared_step, 0)
    lax.fori_loop(0, width // tile, shared_down_step, 0)

    settle(u0)
    combine(u2)
    settle(u1)
    relay(u0)
    s_copy = remote(
        spart.at[1 - tp], spart_in, e_send.at[0], e_recv.at[0], fs, 1 - tp
    )
    s_copy.start()
    combine(u3)
    settle(u2)
    relay(u1)
    settle(u3)
    relay(u2)
    relay(u3)
    for b in UNITS:
        finish(b)
    f_copy = remote(fin.at[1 - tp], fin_in, e_send.at[1], e_recv.at[1], fs, 1 - tp)
    f_copy.start()
    s_copy.wait()
    near = pl.ds(pl.multiple_of(tp * share, share), share)
    far = pl.ds(pl.multiple_of((1 - tp) * share, share), share)
    f_copy.wait()
    for where, value in ((near, fin[tp]), (far, fin_in[...])):
        total = (
            spart[tp, where, :].astype(jnp.float32)
            + spart_in[where, :].astype(jnp.float32)
            + value.astype(jnp.float32)
        )
        out_ref[where, :] = total.astype(jnp.bfloat16)

    own_down.wait()

    def wait_down(i, carry):
        frm = ex.partner(i)
        pltpu.make_async_copy(
            ex.piece(down_v.at[0], frm), ex.piece(sample_down, frm), load_sem.at[0, frm]
        ).wait()
        return carry

    lax.fori_loop(1, 16, wait_down, 0)
    for copy in puts:
        copy.wait()
    chain.drain()
    ex.drain()
    for b in UNITS:
        for copy in d_copies(b):
            copy.wait_send()
        for kind in range(4):
            g_copy(b, kind).wait_send()
        if b > 0:
            pl.when(z < b)(z_copy(b, 0).wait_send)
        if b < 3:
            pl.when(z > b)(z_copy(b, 1).wait_send)


HBM = pl.BlockSpec(memory_space=pl.ANY)
VMEM = pl.BlockSpec(memory_space=pltpu.VMEM)
DMA = pltpu.SemaphoreType.DMA


def gather(tokens_share, dense, gain, raws):
    experts, rows, half = raws[0].shape
    share, width = tokens_share.shape
    n = len(raws)
    weight = jax.ShapeDtypeStruct((experts * rows, half), jnp.bfloat16)
    return pl.pallas_call(
        gather_kernel,
        out_shape=[
            jax.ShapeDtypeStruct((experts, share, width), jnp.bfloat16),
            jax.ShapeDtypeStruct((experts, 1, share), jnp.float32),
        ] + [weight] * (2 * n),
        in_specs=[VMEM] * 3 + [HBM] * n,
        out_specs=[HBM, VMEM] + [HBM] * (2 * n),
        scratch_shapes=[
            pltpu.VMEM((share, width), jnp.bfloat16),
            pltpu.VMEM((n, experts, rows, half), jnp.float32),
            pltpu.VMEM((n, experts, rows, half), jnp.bfloat16),
            DMA((4, 4)), DMA((4,)), DMA((16,)), DMA((16,)), DMA((16,)),
            DMA((n, 16)), DMA((n, 16)), DMA((n, 16)), DMA((n, 16)), DMA((n, 16)), DMA((4,)),
        ],
        compiler_params=pltpu.CompilerParams(
            collective_id=1, has_side_effects=True, vmem_limit_bytes=32 << 20
        ),
        name="gather",
    )(tokens_share, dense, gain, *raws)


def mix(tokens, scale, gain, shared, gathered, weights, down):
    experts, rows, half = down.shape
    tok_rows, width = tokens.shape
    share = tok_rows // 2
    bf16 = jnp.bfloat16
    weight = jax.ShapeDtypeStruct((experts * rows, half), bf16)
    return pl.pallas_call(
        mix_kernel,
        out_shape=[jax.ShapeDtypeStruct((tok_rows, width // 2), bf16)] + [weight] * 4,
        in_specs=[VMEM] * 6 + [HBM] * 6,
        out_specs=[VMEM] + [HBM] * 4,
        scratch_shapes=[
            pltpu.VMEM((4, 4 * share, width), bf16),
            pltpu.VMEM((2, 2, width, half), bf16),
            pltpu.VMEM((2, width, half), bf16),
            pltpu.VMEM((1, experts, rows, half), jnp.float32),
            pltpu.VMEM((1, experts, rows, half), bf16),
            pltpu.VMEM((4, 4 * share, 2 * half), bf16),
            pltpu.VMEM((width, 3 * half), bf16),
            pltpu.VMEM((tok_rows, width), bf16),
            pltpu.VMEM((tok_rows, half), bf16),
            pltpu.VMEM((2, tok_rows, width // 2), bf16),
            pltpu.VMEM((tok_rows, width // 2), bf16),
            pltpu.VMEM((2, share, width // 2), bf16),
            pltpu.VMEM((share, width // 2), bf16),
            pltpu.VMEM((4, share, width // 2), bf16),
            pltpu.VMEM((4, share, width // 2), bf16),
            pltpu.VMEM((4, share, width), bf16),
            pltpu.VMEM((4, share, width), bf16),
            pltpu.VMEM((4, share, width), bf16),
            pltpu.VMEM((4, share, width), bf16),
            DMA((4, 4)), DMA((4,)), DMA((16,)),
            DMA((1, 16)), DMA((1, 16)), DMA((1, 16)), DMA((1, 16)), DMA((1, 16)),
            DMA((2, 4)), DMA((2, 4)), DMA((4, 4)), DMA((4, 4)), DMA((2, 4)), DMA((2, 4)),
            DMA((2,)), DMA((2,)), DMA((8,)),
        ],
        compiler_params=pltpu.CompilerParams(
            collective_id=2, has_side_effects=True, vmem_limit_bytes=67043328
        ),
        name="mix",
    )(tokens, scale, gain, *shared, gathered, *weights, down)


def ring_of(fs_count):
    if fs_count != 16:
        return list(range(fs_count))
    order = []
    for place, column in enumerate((0, 1, 3, 2)):
        heights = range(4) if place % 2 == 0 else range(3, -1, -1)
        order.extend(height * 4 + column for height in heights)
    return order


def reorder(blocks, order):
    if list(order) == list(range(len(order))):
        return blocks
    return jnp.concatenate([blocks[i : i + 1] for i in order], axis=0)


def general_body(
    tokens,
    routes,
    route_weights,
    norm_gain,
    expert_gate,
    expert_up,
    expert_down,
    shared_gate,
    shared_up,
    shared_down,
):
    tp_count = lax.axis_size("tp")
    tp_index = lax.axis_index("tp")
    fs_count = lax.axis_size("fs")
    tok_rows, width = tokens.shape
    experts = expert_gate.shape[0]
    share = tok_rows // tp_count
    own_experts = experts // fs_count
    ring = ring_of(fs_count)
    place_of = [ring.index(i) for i in range(fs_count)]
    groups = None if ring == list(range(fs_count)) else [ring]

    normed = normalize(tokens)
    own_normed = lax.dynamic_slice_in_dim(normed, tp_index * share, share, 0)
    own_routes = lax.dynamic_slice_in_dim(routes, tp_index * share, share, 0)
    own_weights = lax.dynamic_slice_in_dim(route_weights, tp_index * share, share, 0)
    member = own_routes[None, :, :] == jnp.arange(experts, dtype=jnp.int32)[:, None, None]
    dense = jnp.sum(jnp.where(member, own_weights[None, :, :], 0.0), axis=2)
    dense_all = lax.all_gather(dense, "fs", axis=0, tiled=False)
    own_normed, dense_all = lax.optimization_barrier((own_normed, dense_all))
    gathered = lax.all_gather(own_normed, "fs", axis=0, tiled=False)
    gathered = reorder(gathered, ring).reshape(fs_count * share, width)

    gain_rows = norm_gain[None, :, None]
    rounded = (
        (expert_gate * gain_rows).astype(jnp.bfloat16),
        (expert_up * gain_rows).astype(jnp.bfloat16),
        expert_down.astype(jnp.bfloat16),
    )
    sample_gate, sample_up, sample_down = (
        lax.all_to_all(rounded[0], "fs", split_axis=0, concat_axis=1, tiled=True),
        lax.all_to_all(rounded[1], "fs", split_axis=0, concat_axis=1, tiled=True),
        lax.all_to_all(rounded[2], "fs", split_axis=0, concat_axis=1, tiled=True),
    )

    half = shared_gate.shape[1]
    shared_rows = jnp.concatenate(
        [
            (shared_gate * norm_gain[:, None]).astype(jnp.bfloat16),
            (shared_up * norm_gain[:, None]).astype(jnp.bfloat16),
            shared_down.astype(jnp.bfloat16),
        ],
        axis=1,
    )
    common = lax.all_gather(shared_rows, "fs", axis=0, tiled=False, axis_index_groups=groups)
    common_gate, common_up, common_down = (
        reorder(common[:, :, i * half : (i + 1) * half], place_of).reshape(width, half)
        for i in range(3)
    )
    shared_gate_act = jnp.dot(normed, common_gate, preferred_element_type=jnp.float32)
    shared_up_act = jnp.dot(normed, common_up, preferred_element_type=jnp.float32)
    shared_hidden = (jax.nn.silu(shared_gate_act) * shared_up_act).astype(jnp.bfloat16)
    shared_part = jnp.einsum(
        "th,dh->td", shared_hidden, common_down, preferred_element_type=jnp.float32
    ).astype(jnp.bfloat16)
    shared_parts = lax.all_to_all(
        shared_part.reshape(tok_rows, tp_count, width // tp_count).transpose(1, 0, 2),
        "tp",
        split_axis=0,
        concat_axis=0,
        tiled=True,
    )
    shared_sum = jnp.sum(shared_parts.astype(jnp.float32), axis=0)

    scale_all = reorder(
        lax.dynamic_slice_in_dim(
            dense_all, lax.axis_index("fs") * own_experts, own_experts, 1
        ),
        ring,
    )
    total = None
    for expert in range(own_experts):
        scale = scale_all[:, expert, :].reshape(-1)[:, None]
        for shift in range(tp_count):
            gate_w, up_w, down_w = (
                sample_gate[expert],
                sample_up[expert],
                sample_down[expert],
            )
            if shift:
                pairs = [(i, (i + shift) % tp_count) for i in range(tp_count)]
                gate_w, up_w, down_w = (
                    lax.ppermute(gate_w, "tp", pairs),
                    lax.ppermute(up_w, "tp", pairs),
                    lax.ppermute(down_w, "tp", pairs),
                )
            gate = jnp.dot(gathered, gate_w, preferred_element_type=jnp.float32)
            upward = jnp.dot(gathered, up_w, preferred_element_type=jnp.float32)
            hidden = (jax.nn.silu(gate) * upward * scale).astype(jnp.bfloat16)
            part = jnp.einsum("rf,df->rd", hidden, down_w, preferred_element_type=jnp.float32)
            total = part if total is None else total + part
    routed = lax.psum_scatter(
        total.astype(jnp.bfloat16), "fs", scatter_dimension=0, tiled=True, axis_index_groups=groups
    )
    routed = lax.all_to_all(routed, "tp", split_axis=1, concat_axis=0, tiled=True)
    layer_output = (routed.astype(jnp.float32) + shared_sum).astype(jnp.bfloat16)
    return (layer_output, sample_gate, sample_up, sample_down, common_gate, common_up, common_down)

def block_body(
    tokens, routes, route_weights, norm_gain,
    expert_gate, expert_up, expert_down,
    shared_gate, shared_up, shared_down,
):
    tp_index = lax.axis_index("tp")
    tok_rows, width = tokens.shape
    experts = expert_gate.shape[0]
    share = tok_rows // 2
    own_routes = lax.dynamic_slice_in_dim(routes, tp_index * share, share, 0)
    own_weights = lax.dynamic_slice_in_dim(route_weights, tp_index * share, share, 0)
    own_tokens = lax.dynamic_slice_in_dim(tokens, tp_index * share, share, 0)
    member = own_routes[None, :, :] == jnp.arange(experts, dtype=jnp.int32)[:, None, None]
    dense = jnp.sum(jnp.where(member, own_weights[None, :, :], 0.0), axis=2)
    gain = norm_gain[:, None]
    gathered, scale, gate_own, up_own, gate_other, up_other = gather(
        own_tokens, dense[:, None, :], gain, (expert_gate, expert_up)
    )
    layer_output, sample_down, common_gate, common_up, common_down = mix(
        tokens, scale.reshape(experts * share, 1), gain,
        (shared_gate, shared_up, shared_down), gathered.reshape(experts * share, width),
        (gate_own, up_own, gate_other, up_other), expert_down,
    )
    return (
        layer_output, gate_own[None], up_own[None], sample_down[None],
        common_gate, common_up, common_down,
    )


def solution(mesh):
    fits = mesh.shape["fs"] == 16 and mesh.shape["tp"] == 2
    body = block_body if fits else general_body
    return jax.shard_map(
        body,
        mesh=mesh,
        in_specs=(
            P("fs", None),
            P("fs", None),
            P("fs", None),
            P("fs"),
            P(None, "fs", "tp"),
            P(None, "fs", "tp"),
            P(None, "fs", "tp"),
            P("fs", "tp"),
            P("fs", "tp"),
            P("fs", "tp"),
        ),
        out_specs=(
            P("fs", "tp"),
            P("fs", None, "tp"),
            P("fs", None, "tp"),
            P("fs", None, "tp"),
            P(None, "tp"),
            P(None, "tp"),
            P(None, "tp"),
        ),
        check_vma=False,
    )
```

```python
import functools

import jax
import jax.numpy as jnp
from jax import lax
from jax.experimental import pallas as pl
from jax.experimental.pallas import tpu as pltpu
from jax.sharding import PartitionSpec as P

MESH = pl.DeviceIdType.MESH
EPSILON = 1e-06
UNITS = (0, 3, 1, 2)


def normalize(tokens):
    values = tokens.astype(jnp.float32)
    scale = lax.rsqrt(jnp.mean(values * values, axis=-1, keepdims=True) + EPSILON)
    return (values * scale).astype(jnp.bfloat16)


def place():
    fs = lax.axis_index("fs")
    return fs, lax.axis_index("tp"), fs % 2, (fs // 2) % 2, fs // 4


def barrier_all(fs, tp):
    count = lax.axis_size("fs")
    sem = pltpu.get_barrier_semaphore()
    for step in range(1, count):
        pl.semaphore_signal(
            sem, inc=1, device_id=((fs + step) % count, tp), device_id_type=MESH
        )
    pl.semaphore_signal(sem, inc=1, device_id=(fs, 1 - tp), device_id_type=MESH)
    pl.semaphore_wait(sem, count)


def column(row):
    return jnp.transpose(jnp.broadcast_to(row, (row.shape[1], row.shape[1])))[:, 0:1]


def remote(src, dst, ssem, rsem, to, core):
    return pltpu.make_async_remote_copy(
        src_ref=src, dst_ref=dst, send_sem=ssem, recv_sem=rsem,
        device_id=(to, core), device_id_type=MESH,
    )


class Chain:
    def __init__(self, at, send_sem, fwd_sem, recv_sem):
        self.fs, self.tp, self.x, self.y, self.z = place()
        self.at, self.send_sem, self.fwd_sem, self.recv_sem = at, send_sem, fwd_sem, recv_sem
        self.plane = self.fs % 4
        self.xp, self.yp = self.fs + 1 - 2 * self.x, self.fs + 2 - 4 * self.y
        self.xplane, self.yplane = self.plane + 1 - 2 * self.x, self.plane + 2 - 4 * self.y

    def copy(self, slot, sem, to):
        here = self.at(slot)
        return remote(here, here, sem, self.recv_sem.at[slot], to, self.tp)

    def line(self, block, kind):
        z = self.z
        cond = (
            jnp.logical_and(z < 3, block <= z), jnp.logical_and(z > 0, block >= z), None, None
        )[kind]
        to = (self.fs + 4, self.fs - 4, self.xp, self.yp)[kind]
        return cond, self.copy(block * 4 + self.plane, self.send_sem.at[kind, block], to)

    def spread(self, block, kinds=(0, 1, 2, 3)):
        for kind in kinds:
            cond, copy = self.line(block, kind)
            if cond is None:
                copy.start()
            else:
                pl.when(cond)(copy.start)

    def landed(self, slot):
        self.copy(slot, self.send_sem.at[0, 0], self.xp).wait_recv()

    def arrive(self, block, kinds):
        self.landed(block * 4 + self.plane)
        self.spread(block, kinds)

    def forward_copy(self, block, low):
        slot = block * 4 + (self.xplane if low else self.yplane)
        return self.copy(slot, self.fwd_sem.at[block], self.yp if low else self.xp)

    def plane_forward(self, block):
        def forward(low):
            copy = self.forward_copy(block, low)
            copy.wait_recv()
            copy.start()

        if isinstance(block, int):
            forward(block < 2)
            return
        pl.when(jnp.logical_and(block >= 0, block < 2))(lambda: forward(True))
        pl.when(jnp.logical_and(block >= 2, block < 4))(lambda: forward(False))

    def hop(self, step, kinds=(0, 1, 2, 3)):
        z = self.z
        pl.when(z - step - 1 >= 0)(lambda: self.arrive(z - step - 1, kinds))
        pl.when(z + step + 1 < 4)(lambda: self.arrive(z + step + 1, kinds))

    def turn(self, step):
        self.plane_forward(self.z - step)
        if step > 0:
            self.plane_forward(self.z + step)

    def finish(self):
        for block in range(4):
            self.landed(block * 4 + (self.yplane if block < 2 else self.xplane))
            self.landed(block * 4 + 3 - self.plane)

    def drain(self):
        for block in range(4):
            for kind in range(4):
                cond, copy = self.line(block, kind)
                if cond is None:
                    copy.wait_send()
                else:
                    pl.when(cond)(copy.wait_send)
            self.forward_copy(block, block < 2).wait_send()


class Exchange:
    def __init__(self, raw, wide, narrow, own, other, sems):
        self.raw, self.wide, self.narrow, self.own, self.other = raw, wide, narrow, own, other
        self.load_sem, self.send_sem, self.recv_sem, self.psend, self.precv = sems
        self.fs, self.tp, self.x, self.y, self.z = place()
        self.rows = raw[0].shape[1]

    def partner(self, dz, turn, sign=1):
        return (
            ((self.z + 4 + sign * dz) % 4) * 4
            + ((self.y + turn // 2) % 2) * 2
            + (self.x + turn % 2) % 2
        )

    def load(self, t, to):
        return pltpu.make_async_copy(
            self.raw[t].at[to], self.wide.at[to], self.load_sem.at[t, to]
        )

    def each(self, lower, upper, body, sign=1):
        def near(i, carry):
            body(self.partner(0, i, sign))
            return carry

        def far(i, carry):
            k = i - 4
            body(self.partner(1 + (k + 1) % 3, k // 3, sign))
            return carry

        if lower < 4:
            lax.fori_loop(lower, min(upper, 4), near, 0)
        if upper > 4:
            lax.fori_loop(max(lower, 4), min(upper, 16), far, 0)
        if upper > 16:
            body(self.fs)

    def convert(self, t, gain):
        def one(to):
            self.load(t, to).wait()
            block = self.wide[to]
            if gain is not None:
                block = block * gain
            self.narrow[t, to] = block.astype(jnp.bfloat16)
            if t + 1 < len(self.raw):
                self.load(t + 1, to).start()

        self.each(1, 17, one)

    def piece(self, ref, frm):
        return ref.at[pl.ds(frm * self.rows, self.rows)]

    def copy(self, t, to):
        return remote(
            self.narrow.at[t, to], self.piece(self.own[t], self.fs),
            self.send_sem.at[t, to], self.recv_sem.at[t, self.fs], to, self.tp,
        )

    def send(self, lower, upper, tensors):
        def one(to):
            for t in tensors:
                self.copy(t, to).start()

        self.each(lower, upper, one)

    def across(self, t, frm, src):
        return remote(
            src, self.piece(self.other[t], frm), self.psend.at[t, frm], self.precv.at[t, frm],
            self.fs, 1 - self.tp,
        )

    def keep(self, tensors):
        for t in tensors:
            self.own[t][pl.ds(self.fs * self.rows, self.rows), :] = self.narrow[t, self.fs]
            self.across(t, self.fs, self.narrow.at[t, self.fs]).start()

    def pass_on(self, tensors, lower=1, upper=16):
        def one(frm):
            for t in tensors:
                piece = self.piece(self.own[t], frm)
                remote(
                    piece, piece, self.send_sem.at[t, frm], self.recv_sem.at[t, frm], frm, self.tp
                ).wait_recv()
                self.across(t, frm, piece).start()

        self.each(lower, upper, one, -1)

    def finish(self, tensors):
        def one(frm):
            for t in tensors:
                self.across(t, frm, self.piece(self.own[t], frm)).wait()

        self.each(1, 17, one, -1)

    def drain(self):
        def one(to):
            for t in range(len(self.raw)):
                self.copy(t, to).wait_send()

        self.each(1, 16, one)


def dot_nt(a, b):
    return lax.dot_general(a, b, (((1,), (1,)), ((), ())), preferred_element_type=jnp.float32)


def whole_kernel(
    tok_ref, scale_ref, gain_ref, sgate_ref, sup_ref, sdown_ref, gate_ref, up_ref, down_ref,
    out_ref, sample_gate, sample_up, sample_down, common_gate, common_up, common_down,
    acts, gate_up, down_v, wide, narrow, hidden, common, normed, scales, scol,
    shid, spart, spart_in, fin, fin_in, xd_in, yd_in, xg_in, yg_in, zb_in, za_in,
    t_send, t_fwd, t_recv, c_send, c_fwd, c_recv, sc_send, sc_recv,
    load_sem, w_send, w_recv, p_send, p_recv,
    d_send, d_recv, g_send, g_recv, z_send, z_recv, e_send, e_recv, loc_sem,
):
    fs, tp, x, y, z = place()
    rows, half = sgate_ref.shape
    width = tok_ref.shape[1]
    share = acts.shape[1] // 4
    ex = Exchange(
        (gate_ref, up_ref, down_ref), wide, narrow,
        (gate_up.at[0, 0], gate_up.at[1, 0], down_v.at[0]),
        (gate_up.at[0, 1], gate_up.at[1, 1], down_v.at[1]),
        (load_sem, w_send, w_recv, p_send, p_recv),
    )
    tokens = Chain(
        lambda slot: acts.at[slot // 4, pl.ds((slot % 4) * share, share)], t_send, t_fwd, t_recv
    )
    chain = Chain(lambda slot: common.at[pl.ds(slot * rows, rows)], c_send, c_fwd, c_recv)

    ex.each(1, 17, lambda to: ex.load(0, to).start())
    gain = column(gain_ref[...])
    mine = pl.ds(fs * rows, rows)
    common[mine, 0:half] = (sgate_ref[...] * gain).astype(jnp.bfloat16)
    common[mine, half : 2 * half] = (sup_ref[...] * gain).astype(jnp.bfloat16)
    common[mine, 2 * half : 3 * half] = sdown_ref[...].astype(jnp.bfloat16)
    normed[...] = normalize(tok_ref[...])
    acts[z, pl.ds((fs % 4) * share, share), :] = normed[
        pl.ds(pl.multiple_of(tp * share, share), share), :
    ]
    ex.convert(0, gain)
    ex.convert(1, gain)
    ex.convert(2, None)
    barrier_all(fs, tp)

    tokens.spread(z)

    def scale_copy(to):
        return remote(
            scale_ref.at[to, tp], scales.at[fs], sc_send.at[to], sc_recv.at[fs], to, tp
        )

    own_scale = pltpu.make_async_copy(scale_ref.at[fs, tp], scales.at[fs], loc_sem.at[0])
    own_scale.start()
    ex.each(1, 16, lambda to: scale_copy(to).start())
    ex.send(1, 5, (0, 1))
    tokens.hop(0)
    tokens.turn(0)
    ex.send(5, 6, (0, 1))
    tokens.hop(1)
    tokens.turn(1)
    tokens.hop(2)
    along = (0, 1)
    chain.spread(z, along)
    ex.send(6, 9, (0, 1))
    tokens.turn(2)
    chain.hop(0, along)
    ex.send(9, 12, (0, 1))
    chain.hop(1, along)
    ex.send(12, 16, (0, 1))
    ex.send(4, 16, (2,))
    tokens.turn(3)
    chain.hop(2, along)
    ex.send(1, 4, (2,))
    for block in range(4):
        chain.spread(block, (2, 3))
    ex.keep((0, 1, 2))
    own_scale.wait()

    def take_scale(frm):
        here = scales.at[frm]
        remote(here, here, sc_send.at[frm], sc_recv.at[frm], frm, tp).wait_recv()
        scale_copy(frm).wait_send()

    ex.each(1, 16, take_scale)
    for slot in range(16):
        scol[pl.ds(slot * share, share), :] = column(scales[slot])
    ex.pass_on((0, 1))
    ex.finish((0, 1))
    samples = [
        pltpu.make_async_copy(gate_up.at[t, 0], ref, loc_sem.at[1 + t])
        for t, ref in enumerate((sample_gate, sample_up))
    ]
    for copy in samples:
        copy.start()
    tokens.finish()

    tile = 256
    per_half = half // tile

    def gate_up_unit(b):
        def step(j, carry):
            h, c = j // per_half, j % per_half
            cols = pl.ds(pl.multiple_of(c * tile, tile), tile)
            a = acts[b]
            gate = jnp.dot(a, gate_up[0, h, :, cols], preferred_element_type=jnp.float32)
            up = jnp.dot(a, gate_up[1, h, :, cols], preferred_element_type=jnp.float32)
            scale = scol[pl.ds(b * 4 * share, 4 * share), :]
            hidden[b, :, pl.ds(pl.multiple_of(j * tile, tile), tile)] = (
                jax.nn.silu(gate) * up * scale
            ).astype(jnp.bfloat16)
            return carry

        lax.fori_loop(0, 2 * per_half, step, 0)

    for b in UNITS:
        gate_up_unit(b)
    tokens.drain()
    chain.plane_forward(0)
    chain.plane_forward(1)

    ex.pass_on((2,))
    ex.finish((2,))
    samples.append(pltpu.make_async_copy(down_v.at[0], sample_down, loc_sem.at[3]))
    samples[-1].start()

    plane = fs % 4
    xp, yp = chain.xp, chain.yp
    xplane, yplane, dplane = chain.xplane, chain.yplane, 3 - plane
    mid, quarter = width // 2, width // 4

    def columns(side):
        return pl.ds(side * mid, quarter), pl.ds(side * mid + quarter, quarter)

    def part(b, which, cols):
        return acts.at[b, pl.ds(which * share, share), cols]

    def down_unit(b, side):
        def step(n, carry):
            cols = pl.ds(pl.multiple_of(side * mid + n * tile, tile), tile)
            acts[b, :, cols] = (
                dot_nt(hidden[b, :, 0:half], down_v[0, cols, :])
                + dot_nt(hidden[b, :, half : 2 * half], down_v[1, cols, :])
            ).astype(jnp.bfloat16)
            return carry

        lax.fori_loop(0, mid // tile, step, 0)

    def d_copies(b, side):
        lo, hi = columns(side)
        box = pl.ds(side * quarter, quarter)
        n = 2 * b + side
        return (
            remote(
                part(b, dplane, lo), xd_in.at[b, :, box], d_send.at[0, n], d_recv.at[0, n], xp, tp
            ),
            remote(
                part(b, dplane, hi), yd_in.at[b, :, box], d_send.at[1, n], d_recv.at[1, n], yp, tp
            ),
        )

    def g_copy(b, side, kind):
        lo, hi = columns(side)
        which, cols, box, to = (
            (xplane, lo, xg_in, xp),
            (xplane, hi, xg_in, xp),
            (yplane, hi, yg_in, yp),
            (yplane, lo, yg_in, yp),
        )[kind]
        n = 2 * b + side
        return remote(
            part(b, which, cols), box.at[b, :, cols], g_send.at[kind, n], g_recv.at[kind, n],
            to, tp,
        )

    def first(b, side):
        for copy in d_copies(b, side):
            copy.start()
        g_copy(b, side, 0).start()
        g_copy(b, side, 2).start()

    def add_into(ref, others):
        total = ref[...].astype(jnp.float32)
        for other in others:
            total = total + other[...].astype(jnp.float32)
        ref[...] = total.astype(jnp.bfloat16)

    def combine(b, side):
        lo, hi = columns(side)
        box = pl.ds(side * quarter, quarter)
        x_copy, y_copy = d_copies(b, side)
        x_copy.wait_recv()
        add_into(part(b, yplane, lo), [xd_in.at[b, :, box]])
        g_copy(b, side, 3).start()
        y_copy.wait_recv()
        add_into(part(b, xplane, hi), [yd_in.at[b, :, box]])
        g_copy(b, side, 1).start()

    def z_copy(b, side, way):
        box = (zb_in, za_in)[way]
        cols = pl.ds(side * mid, mid)
        n = 2 * b + side
        return remote(
            part(b, plane, cols), box.at[b, :, cols], z_send.at[way, n], z_recv.at[way, n],
            fs + (4, -4)[way], tp,
        )

    def settle(b, side):
        cols = pl.ds(side * mid, mid)
        for kind in range(4):
            g_copy(b, side, kind).wait_recv()
        add_into(part(b, plane, cols), [xg_in.at[b, :, cols], yg_in.at[b, :, cols]])
        if b > 0:
            pl.when(z == 0)(z_copy(b, side, 0).start)
        if b < 3:
            pl.when(z == 3)(z_copy(b, side, 1).start)

    def relay(b, side):
        cols = pl.ds(side * mid, mid)
        if b > 0:
            @pl.when(jnp.logical_and(z > 0, z < b))
            def _():
                z_copy(b, side, 0).wait_recv()
                add_into(part(b, plane, cols), [zb_in.at[b, :, cols]])
                z_copy(b, side, 0).start()

        if b < 3:
            @pl.when(jnp.logical_and(z < 3, z > b))
            def _():
                z_copy(b, side, 1).wait_recv()
                add_into(part(b, plane, cols), [za_in.at[b, :, cols]])
                z_copy(b, side, 1).start()

    def finish(b):
        @pl.when(z == b)
        def _():
            for side in range(2):
                cols = pl.ds(side * mid, mid)
                total = acts[b, pl.ds(plane * share, share), cols].astype(jnp.float32)
                if b > 0:
                    z_copy(b, side, 0).wait_recv()
                    total = total + zb_in[b, :, cols].astype(jnp.float32)
                if b < 3:
                    z_copy(b, side, 1).wait_recv()
                    total = total + za_in[b, :, cols].astype(jnp.float32)
                fin[side] = total.astype(jnp.bfloat16)

    puts = [
        pltpu.make_async_copy(common.at[:, pl.ds(i * half, half)], ref, loc_sem.at[4 + i])
        for i, ref in enumerate((common_gate, common_up, common_down))
    ]

    def shared_step(c, carry):
        a = normed[...]
        cols = pl.ds(pl.multiple_of(c * tile, tile), tile)
        gate = jnp.dot(a, common[:, cols], preferred_element_type=jnp.float32)
        up = jnp.dot(
            a, common[:, pl.ds(pl.multiple_of(half + c * tile, tile), tile)],
            preferred_element_type=jnp.float32,
        )
        shid[:, cols] = (jax.nn.silu(gate) * up).astype(jnp.bfloat16)
        return carry

    def shared_down_step(n, carry):
        per = mid // tile
        spart[n // per, :, pl.ds(pl.multiple_of((n % per) * tile, tile), tile)] = dot_nt(
            shid[...],
            common[pl.ds(pl.multiple_of(n * tile, tile), tile), 2 * half : 3 * half],
        ).astype(jnp.bfloat16)
        return carry

    s_copy = remote(spart.at[1 - tp], spart_in, e_send.at[0], e_recv.at[0], fs, 1 - tp)

    def shared_expert():
        chain.finish()
        for copy in puts:
            copy.start()
        lax.fori_loop(0, per_half, shared_step, 0)
        lax.fori_loop(0, width // tile, shared_down_step, 0)
        s_copy.start()

    pieces = [(b, side) for b in UNITS for side in range(2)]
    count = len(pieces)
    for i in range(count + 4):
        if i < count:
            down_unit(*pieces[i])
            first(*pieces[i])
        if i == 1:
            chain.plane_forward(2)
        if i == 2:
            chain.plane_forward(3)
        if i == count + 1:
            shared_expert()
        if 1 <= i <= count:
            combine(*pieces[i - 1])
        if 2 <= i <= count + 1:
            settle(*pieces[i - 2])
        if i >= 4:
            relay(*pieces[i - 4])
    for b in UNITS:
        finish(b)
    f_copy = remote(fin.at[1 - tp], fin_in, e_send.at[1], e_recv.at[1], fs, 1 - tp)
    f_copy.start()
    s_copy.wait()
    near = pl.ds(pl.multiple_of(tp * share, share), share)
    far = pl.ds(pl.multiple_of((1 - tp) * share, share), share)
    f_copy.wait()
    for where, value in ((near, fin[tp]), (far, fin_in[...])):
        total = (
            spart[tp, where, :].astype(jnp.float32)
            + spart_in[where, :].astype(jnp.float32)
            + value.astype(jnp.float32)
        )
        out_ref[where, :] = total.astype(jnp.bfloat16)

    for copy in samples:
        copy.wait()
    for copy in puts:
        copy.wait()
    chain.drain()
    ex.drain()
    for b, side in pieces:
        for copy in d_copies(b, side):
            copy.wait_send()
        for kind in range(4):
            g_copy(b, side, kind).wait_send()
        if b > 0:
            pl.when(z < b)(z_copy(b, side, 0).wait_send)
        if b < 3:
            pl.when(z > b)(z_copy(b, side, 1).wait_send)


HBM = pl.BlockSpec(memory_space=pl.ANY)
VMEM = pl.BlockSpec(memory_space=pltpu.VMEM)
DMA = pltpu.SemaphoreType.DMA


def whole(tokens, scale, gain, shared, raw):
    experts, rows, half = raw[0].shape
    tok_rows, width = tokens.shape
    share = tok_rows // 2
    bf16, f32 = jnp.bfloat16, jnp.float32
    weight = jax.ShapeDtypeStruct((experts * rows, half), bf16)
    return pl.pallas_call(
        whole_kernel,
        out_shape=[jax.ShapeDtypeStruct((tok_rows, width // 2), bf16)] + [weight] * 6,
        in_specs=[VMEM] * 6 + [HBM] * 3,
        out_specs=[VMEM] + [HBM] * 6,
        scratch_shapes=[
            pltpu.VMEM((4, 4 * share, width), bf16),
            pltpu.VMEM((2, 2, width, half), bf16),
            pltpu.VMEM((2, width, half), bf16),
            pltpu.VMEM((experts, rows, half), f32),
            pltpu.VMEM((3, experts, rows, half), bf16),
            pltpu.VMEM((4, 4 * share, 2 * half), bf16),
            pltpu.VMEM((width, 3 * half), bf16),
            pltpu.VMEM((tok_rows, width), bf16),
            pltpu.VMEM((experts, 1, share), f32),
            pltpu.VMEM((experts * share, 1), f32),
            pltpu.VMEM((tok_rows, half), bf16),
            pltpu.VMEM((2, tok_rows, width // 2), bf16),
            pltpu.VMEM((tok_rows, width // 2), bf16),
            pltpu.VMEM((2, share, width // 2), bf16),
            pltpu.VMEM((share, width // 2), bf16),
            pltpu.VMEM((4, share, width // 2), bf16),
            pltpu.VMEM((4, share, width // 2), bf16),
            pltpu.VMEM((4, share, width), bf16),
            pltpu.VMEM((4, share, width), bf16),
            pltpu.VMEM((4, share, width), bf16),
            pltpu.VMEM((4, share, width), bf16),
            DMA((4, 4)), DMA((4,)), DMA((16,)), DMA((4, 4)), DMA((4,)), DMA((16,)),
            DMA((16,)), DMA((16,)),
            DMA((3, 16)), DMA((3, 16)), DMA((3, 16)), DMA((3, 16)), DMA((3, 16)),
            DMA((2, 8)), DMA((2, 8)), DMA((4, 8)), DMA((4, 8)), DMA((2, 8)), DMA((2, 8)),
            DMA((2,)), DMA((2,)), DMA((8,)),
        ],
        compiler_params=pltpu.CompilerParams(
            collective_id=1, has_side_effects=True, vmem_limit_bytes=67043328
        ),
        name="whole",
    )(tokens, scale, gain, *shared, *raw)


def emit_kernel(count, *refs):
    source, target, boxes = refs[:count], refs[count : 2 * count], refs[2 * count : -2]
    in_sem, out_sem = refs[-2:]
    parts = []
    for i in range(count):
        length = source[i].shape[0] // 4
        for c in range(4):
            at = pl.ds(c * length, length)
            parts.append((
                pltpu.make_async_copy(source[i].at[at], boxes[i].at[at], in_sem.at[i, c]),
                pltpu.make_async_copy(boxes[i].at[at], target[i].at[at], out_sem.at[i, c]),
            ))
    for load, _ in parts:
        load.start()
    for load, store in parts:
        load.wait()
        store.start()
    for _, store in parts:
        store.wait()


def emit(*arrays):
    n = len(arrays)
    shapes = [jax.ShapeDtypeStruct(a.shape, a.dtype) for a in arrays]
    return pl.pallas_call(
        functools.partial(emit_kernel, n),
        out_shape=shapes,
        in_specs=[HBM] * n,
        out_specs=[HBM] * n,
        scratch_shapes=[pltpu.VMEM(a.shape, a.dtype) for a in arrays]
        + [DMA((n, 4)), DMA((n, 4))],
        compiler_params=pltpu.CompilerParams(vmem_limit_bytes=67043328),
        name="emit",
    )(*arrays)


def ring_of(fs_count):
    if fs_count != 16:
        return list(range(fs_count))
    order = []
    for place, column in enumerate((0, 1, 3, 2)):
        heights = range(4) if place % 2 == 0 else range(3, -1, -1)
        order.extend(height * 4 + column for height in heights)
    return order


def reorder(blocks, order):
    if list(order) == list(range(len(order))):
        return blocks
    return jnp.concatenate([blocks[i : i + 1] for i in order], axis=0)


def general_body(
    tokens,
    routes,
    route_weights,
    norm_gain,
    expert_gate,
    expert_up,
    expert_down,
    shared_gate,
    shared_up,
    shared_down,
):
    tp_count = lax.axis_size("tp")
    tp_index = lax.axis_index("tp")
    fs_count = lax.axis_size("fs")
    tok_rows, width = tokens.shape
    experts = expert_gate.shape[0]
    share = tok_rows // tp_count
    own_experts = experts // fs_count
    ring = ring_of(fs_count)
    place_of = [ring.index(i) for i in range(fs_count)]
    groups = None if ring == list(range(fs_count)) else [ring]

    normed = normalize(tokens)
    own_normed = lax.dynamic_slice_in_dim(normed, tp_index * share, share, 0)
    own_routes = lax.dynamic_slice_in_dim(routes, tp_index * share, share, 0)
    own_weights = lax.dynamic_slice_in_dim(route_weights, tp_index * share, share, 0)
    member = own_routes[None, :, :] == jnp.arange(experts, dtype=jnp.int32)[:, None, None]
    dense = jnp.sum(jnp.where(member, own_weights[None, :, :], 0.0), axis=2)
    dense_all = lax.all_gather(dense, "fs", axis=0, tiled=False)
    own_normed, dense_all = lax.optimization_barrier((own_normed, dense_all))
    gathered = lax.all_gather(own_normed, "fs", axis=0, tiled=False)
    gathered = reorder(gathered, ring).reshape(fs_count * share, width)

    gain_rows = norm_gain[None, :, None]
    rounded = (
        (expert_gate * gain_rows).astype(jnp.bfloat16),
        (expert_up * gain_rows).astype(jnp.bfloat16),
        expert_down.astype(jnp.bfloat16),
    )
    sample_gate, sample_up, sample_down = (
        lax.all_to_all(rounded[0], "fs", split_axis=0, concat_axis=1, tiled=True),
        lax.all_to_all(rounded[1], "fs", split_axis=0, concat_axis=1, tiled=True),
        lax.all_to_all(rounded[2], "fs", split_axis=0, concat_axis=1, tiled=True),
    )

    half = shared_gate.shape[1]
    shared_rows = jnp.concatenate(
        [
            (shared_gate * norm_gain[:, None]).astype(jnp.bfloat16),
            (shared_up * norm_gain[:, None]).astype(jnp.bfloat16),
            shared_down.astype(jnp.bfloat16),
        ],
        axis=1,
    )
    common = lax.all_gather(shared_rows, "fs", axis=0, tiled=False, axis_index_groups=groups)
    common_gate, common_up, common_down = (
        reorder(common[:, :, i * half : (i + 1) * half], place_of).reshape(width, half)
        for i in range(3)
    )
    shared_gate_act = jnp.dot(normed, common_gate, preferred_element_type=jnp.float32)
    shared_up_act = jnp.dot(normed, common_up, preferred_element_type=jnp.float32)
    shared_hidden = (jax.nn.silu(shared_gate_act) * shared_up_act).astype(jnp.bfloat16)
    shared_part = jnp.einsum(
        "th,dh->td", shared_hidden, common_down, preferred_element_type=jnp.float32
    ).astype(jnp.bfloat16)
    shared_parts = lax.all_to_all(
        shared_part.reshape(tok_rows, tp_count, width // tp_count).transpose(1, 0, 2),
        "tp",
        split_axis=0,
        concat_axis=0,
        tiled=True,
    )
    shared_sum = jnp.sum(shared_parts.astype(jnp.float32), axis=0)

    scale_all = reorder(
        lax.dynamic_slice_in_dim(
            dense_all, lax.axis_index("fs") * own_experts, own_experts, 1
        ),
        ring,
    )
    total = None
    for expert in range(own_experts):
        scale = scale_all[:, expert, :].reshape(-1)[:, None]
        for shift in range(tp_count):
            gate_w, up_w, down_w = (
                sample_gate[expert],
                sample_up[expert],
                sample_down[expert],
            )
            if shift:
                pairs = [(i, (i + shift) % tp_count) for i in range(tp_count)]
                gate_w, up_w, down_w = (
                    lax.ppermute(gate_w, "tp", pairs),
                    lax.ppermute(up_w, "tp", pairs),
                    lax.ppermute(down_w, "tp", pairs),
                )
            gate = jnp.dot(gathered, gate_w, preferred_element_type=jnp.float32)
            upward = jnp.dot(gathered, up_w, preferred_element_type=jnp.float32)
            hidden = (jax.nn.silu(gate) * upward * scale).astype(jnp.bfloat16)
            part = jnp.einsum("rf,df->rd", hidden, down_w, preferred_element_type=jnp.float32)
            total = part if total is None else total + part
    routed = lax.psum_scatter(
        total.astype(jnp.bfloat16), "fs", scatter_dimension=0, tiled=True, axis_index_groups=groups
    )
    routed = lax.all_to_all(routed, "tp", split_axis=1, concat_axis=0, tiled=True)
    layer_output = (routed.astype(jnp.float32) + shared_sum).astype(jnp.bfloat16)
    return (layer_output, sample_gate, sample_up, sample_down, common_gate, common_up, common_down)

def block_body(
    tokens, routes, route_weights, norm_gain,
    expert_gate, expert_up, expert_down,
    shared_gate, shared_up, shared_down,
):
    tok_rows = tokens.shape[0]
    experts = expert_gate.shape[0]
    share = tok_rows // 2
    member = routes[None, :, :] == jnp.arange(experts, dtype=jnp.int32)[:, None, None]
    dense = jnp.sum(jnp.where(member, route_weights[None, :, :], 0.0), axis=2)
    gain = norm_gain[None, :]
    outputs = whole(
        tokens, dense.reshape(experts, 2, 1, share), gain,
        (shared_gate, shared_up, shared_down), (expert_gate, expert_up, expert_down),
    )
    (
        layer_output, sample_gate, sample_up, sample_down, common_gate, common_up, common_down
    ) = emit(*outputs)
    return (
        layer_output, sample_gate[None], sample_up[None], sample_down[None],
        common_gate, common_up, common_down,
    )


def solution(mesh):
    fits = mesh.shape["fs"] == 16 and mesh.shape["tp"] == 2
    body = block_body if fits else general_body
    return jax.shard_map(
        body,
        mesh=mesh,
        in_specs=(
            P("fs", None),
            P("fs", None),
            P("fs", None),
            P("fs"),
            P(None, "fs", "tp"),
            P(None, "fs", "tp"),
            P(None, "fs", "tp"),
            P("fs", "tp"),
            P("fs", "tp"),
            P("fs", "tp"),
        ),
        out_specs=(
            P("fs", "tp"),
            P("fs", None, "tp"),
            P("fs", None, "tp"),
            P("fs", None, "tp"),
            P(None, "tp"),
            P(None, "tp"),
            P(None, "tp"),
        ),
        check_vma=False,
    )
```

```python
import functools

import jax
import jax.numpy as jnp
from jax import lax
from jax.experimental import pallas as pl
from jax.experimental.pallas import tpu as pltpu
from jax.sharding import PartitionSpec as P

MESH = pl.DeviceIdType.MESH
EPSILON = 1e-06
UNITS = (0, 3, 1, 2)


def normalize(tokens):
    values = tokens.astype(jnp.float32)
    scale = lax.rsqrt(jnp.mean(values * values, axis=-1, keepdims=True) + EPSILON)
    return (values * scale).astype(jnp.bfloat16)


def place():
    fs = lax.axis_index("fs")
    return fs, lax.axis_index("tp"), fs % 2, (fs // 2) % 2, fs // 4


def greet(fs, tp):
    count = lax.axis_size("fs")
    sem = pltpu.get_barrier_semaphore()
    for step in range(1, count):
        pl.semaphore_signal(
            sem, inc=1, device_id=((fs + step) % count, tp), device_id_type=MESH
        )
    pl.semaphore_signal(sem, inc=1, device_id=(fs, 1 - tp), device_id_type=MESH)


def meet():
    pl.semaphore_wait(pltpu.get_barrier_semaphore(), lax.axis_size("fs"))


def column(row):
    return jnp.transpose(jnp.broadcast_to(row, (row.shape[1], row.shape[1])))[:, 0:1]


def remote(src, dst, ssem, rsem, to, core):
    return pltpu.make_async_remote_copy(
        src_ref=src, dst_ref=dst, send_sem=ssem, recv_sem=rsem,
        device_id=(to, core), device_id_type=MESH,
    )


class Chain:
    def __init__(self, at, send_sem, fwd_sem, recv_sem):
        self.fs, self.tp, self.x, self.y, self.z = place()
        self.at, self.send_sem, self.fwd_sem, self.recv_sem = at, send_sem, fwd_sem, recv_sem
        self.plane = self.fs % 4
        self.xp, self.yp = self.fs + 1 - 2 * self.x, self.fs + 2 - 4 * self.y
        self.xplane, self.yplane = self.plane + 1 - 2 * self.x, self.plane + 2 - 4 * self.y

    def copy(self, slot, sem, to):
        here = self.at(slot)
        return remote(here, here, sem, self.recv_sem.at[slot], to, self.tp)

    def line(self, block, kind):
        z = self.z
        cond = (
            jnp.logical_and(z < 3, block <= z), jnp.logical_and(z > 0, block >= z), None, None
        )[kind]
        to = (self.fs + 4, self.fs - 4, self.xp, self.yp)[kind]
        return cond, self.copy(block * 4 + self.plane, self.send_sem.at[kind, block], to)

    def spread(self, block, kinds=(0, 1, 2, 3)):
        for kind in kinds:
            cond, copy = self.line(block, kind)
            if cond is None:
                copy.start()
            else:
                pl.when(cond)(copy.start)

    def landed(self, slot):
        self.copy(slot, self.send_sem.at[0, 0], self.xp).wait_recv()

    def arrive(self, block, kinds):
        self.landed(block * 4 + self.plane)
        self.spread(block, kinds)

    def forward_copy(self, block, low):
        slot = block * 4 + (self.xplane if low else self.yplane)
        return self.copy(slot, self.fwd_sem.at[block], self.yp if low else self.xp)

    def plane_forward(self, block):
        def forward(low):
            copy = self.forward_copy(block, low)
            copy.wait_recv()
            copy.start()

        if isinstance(block, int):
            forward(block < 2)
            return
        pl.when(jnp.logical_and(block >= 0, block < 2))(lambda: forward(True))
        pl.when(jnp.logical_and(block >= 2, block < 4))(lambda: forward(False))

    def hop(self, step, kinds=(0, 1, 2, 3)):
        z = self.z
        pl.when(z - step - 1 >= 0)(lambda: self.arrive(z - step - 1, kinds))
        pl.when(z + step + 1 < 4)(lambda: self.arrive(z + step + 1, kinds))

    def fan(self, step):
        z = self.z
        pl.when(z - step >= 0)(lambda: self.spread(z - step, (2, 3)))
        if step > 0:
            pl.when(z + step < 4)(lambda: self.spread(z + step, (2, 3)))

    def turn(self, step):
        self.plane_forward(self.z - step)
        if step > 0:
            self.plane_forward(self.z + step)

    def finish(self):
        for block in range(4):
            self.landed(block * 4 + (self.yplane if block < 2 else self.xplane))
            self.landed(block * 4 + 3 - self.plane)

    def drain(self):
        for block in range(4):
            for kind in range(4):
                cond, copy = self.line(block, kind)
                if cond is None:
                    copy.wait_send()
                else:
                    pl.when(cond)(copy.wait_send)
            self.forward_copy(block, block < 2).wait_send()


class Exchange:
    def __init__(self, raw, wide, narrow, own, other, sems):
        self.raw, self.wide, self.narrow, self.own, self.other = raw, wide, narrow, own, other
        self.load_sem, self.send_sem, self.recv_sem, self.psend, self.precv = sems
        self.fs, self.tp, self.x, self.y, self.z = place()
        self.rows = raw[0].shape[1]

    def partner(self, dz, turn, sign=1):
        return (
            ((self.z + 4 + sign * dz) % 4) * 4
            + ((self.y + turn // 2) % 2) * 2
            + (self.x + turn % 2) % 2
        )

    def load(self, t, to):
        return pltpu.make_async_copy(
            self.raw[t].at[to], self.wide.at[to], self.load_sem.at[t, to]
        )

    def each(self, lower, upper, body, sign=1):
        def near(i, carry):
            body(self.partner(0, i, sign))
            return carry

        def far(i, carry):
            k = i - 4
            body(self.partner(1 + (k + 1) % 3, k // 3, sign))
            return carry

        if lower < 4:
            lax.fori_loop(lower, min(upper, 4), near, 0)
        if upper > 4:
            lax.fori_loop(max(lower, 4), min(upper, 16), far, 0)
        if upper > 16:
            body(self.fs)

    def convert(self, t, gain):
        def one(to):
            self.load(t, to).wait()
            block = self.wide[to]
            if gain is not None:
                block = block * gain
            self.narrow[t, to] = block.astype(jnp.bfloat16)
            if t + 1 < len(self.raw):
                self.load(t + 1, to).start()

        self.each(1, 17, one)

    def piece(self, ref, frm):
        return ref.at[pl.ds(frm * self.rows, self.rows)]

    def copy(self, t, to):
        return remote(
            self.narrow.at[t, to], self.piece(self.own[t], self.fs),
            self.send_sem.at[t, to], self.recv_sem.at[t, self.fs], to, self.tp,
        )

    def send(self, lower, upper, tensors):
        def one(to):
            for t in tensors:
                self.copy(t, to).start()

        self.each(lower, upper, one)

    def across(self, t, frm, src):
        return remote(
            src, self.piece(self.other[t], frm), self.psend.at[t, frm], self.precv.at[t, frm],
            self.fs, 1 - self.tp,
        )

    def keep(self, tensors):
        for t in tensors:
            self.own[t][pl.ds(self.fs * self.rows, self.rows), :] = self.narrow[t, self.fs]
            self.across(t, self.fs, self.narrow.at[t, self.fs]).start()

    def pass_on(self, tensors, lower=1, upper=16):
        def one(frm):
            for t in tensors:
                piece = self.piece(self.own[t], frm)
                remote(
                    piece, piece, self.send_sem.at[t, frm], self.recv_sem.at[t, frm], frm, self.tp
                ).wait_recv()
                self.across(t, frm, piece).start()

        self.each(lower, upper, one, -1)

    def finish(self, tensors):
        def one(frm):
            for t in tensors:
                self.across(t, frm, self.piece(self.own[t], frm)).wait()

        self.each(1, 17, one, -1)

    def drain(self):
        def one(to):
            for t in range(len(self.raw)):
                self.copy(t, to).wait_send()

        self.each(1, 16, one)


def dot_nt(a, b):
    return lax.dot_general(a, b, (((1,), (1,)), ((), ())), preferred_element_type=jnp.float32)


def whole_kernel(
    tok_ref, scale_ref, gain_ref, sgate_ref, sup_ref, sdown_ref, gate_ref, up_ref, down_ref,
    out_ref, sample_gate, sample_up, sample_down, common_gate, common_up, common_down,
    acts, gate_up, down_v, wide, narrow, hidden, common, normed, scales, scol,
    shid, spart, spart_in, fin, fin_in, xd_in, yd_in, xg_in, yg_in, zb_in, za_in, lb_in, la_in,
    t_send, t_fwd, t_recv, c_send, c_fwd, c_recv, sc_send, sc_recv,
    load_sem, w_send, w_recv, p_send, p_recv,
    d_send, d_recv, g_send, g_recv, z_send, z_recv, l_send, l_recv, e_send, e_recv, loc_sem,
):
    fs, tp, x, y, z = place()
    rows, half = sgate_ref.shape
    width = tok_ref.shape[1]
    share = acts.shape[1] // 4
    ex = Exchange(
        (gate_ref, up_ref, down_ref), wide, narrow,
        (gate_up.at[0, 0], gate_up.at[1, 0], down_v.at[0]),
        (gate_up.at[0, 1], gate_up.at[1, 1], down_v.at[1]),
        (load_sem, w_send, w_recv, p_send, p_recv),
    )
    tokens = Chain(
        lambda slot: acts.at[slot // 4, pl.ds((slot % 4) * share, share)], t_send, t_fwd, t_recv
    )
    chain = Chain(lambda slot: common.at[pl.ds(slot * rows, rows)], c_send, c_fwd, c_recv)

    greet(fs, tp)
    own_tokens = pltpu.make_async_copy(tok_ref, normed, loc_sem.at[7])
    own_tokens.start()
    ex.each(1, 17, lambda to: ex.load(0, to).start())
    own_tokens.wait()
    normed[...] = normalize(normed[...])
    acts[z, pl.ds((fs % 4) * share, share), :] = normed[
        pl.ds(pl.multiple_of(tp * share, share), share), :
    ]
    gain = column(gain_ref[...])
    mine = pl.ds(fs * rows, rows)
    common[mine, 0:half] = (sgate_ref[...] * gain).astype(jnp.bfloat16)
    common[mine, half : 2 * half] = (sup_ref[...] * gain).astype(jnp.bfloat16)
    common[mine, 2 * half : 3 * half] = sdown_ref[...].astype(jnp.bfloat16)
    meet()

    tokens.spread(z)
    ex.convert(0, gain)
    ex.convert(1, gain)

    def scale_copy(to):
        return remote(
            scale_ref.at[to, tp], scales.at[fs], sc_send.at[to], sc_recv.at[fs], to, tp
        )

    own_scale = pltpu.make_async_copy(scale_ref.at[fs, tp], scales.at[fs], loc_sem.at[0])
    own_scale.start()
    ex.each(1, 16, lambda to: scale_copy(to).start())
    ex.send(1, 5, (0, 1))
    ex.convert(2, None)
    tokens.hop(0)
    tokens.turn(0)
    ex.send(5, 6, (0, 1))
    tokens.hop(1)
    tokens.turn(1)
    tokens.hop(2)
    along = (0, 1)
    chain.spread(z, along)
    ex.send(6, 9, (0, 1))
    tokens.turn(2)
    chain.hop(0, along)
    ex.send(9, 12, (0, 1))
    chain.hop(1, along)
    ex.send(12, 16, (0, 1))
    ex.send(4, 16, (2,))
    tokens.turn(3)
    for step in range(3):
        chain.fan(step)
    chain.hop(2, along)
    chain.fan(3)
    ex.send(1, 4, (2,))
    ex.keep((0, 1, 2))
    own_scale.wait()

    def take_scale(frm):
        here = scales.at[frm]
        remote(here, here, sc_send.at[frm], sc_recv.at[frm], frm, tp).wait_recv()
        scale_copy(frm).wait_send()

    ex.each(1, 16, take_scale)
    for slot in range(16):
        scol[pl.ds(slot * share, share), :] = column(scales[slot])
    ex.pass_on((0, 1))
    ex.finish((0, 1))
    samples = [
        pltpu.make_async_copy(gate_up.at[t, 0], ref, loc_sem.at[1 + t])
        for t, ref in enumerate((sample_gate, sample_up))
    ]
    for copy in samples:
        copy.start()
    tokens.finish()

    tile = 256
    per_half = half // tile

    def gate_up_unit(b):
        def step(j, carry):
            h, c = j // per_half, j % per_half
            cols = pl.ds(pl.multiple_of(c * tile, tile), tile)
            a = acts[b]
            gate = jnp.dot(a, gate_up[0, h, :, cols], preferred_element_type=jnp.float32)
            up = jnp.dot(a, gate_up[1, h, :, cols], preferred_element_type=jnp.float32)
            scale = scol[pl.ds(b * 4 * share, 4 * share), :]
            hidden[b, :, pl.ds(pl.multiple_of(j * tile, tile), tile)] = (
                jax.nn.silu(gate) * up * scale
            ).astype(jnp.bfloat16)
            return carry

        lax.fori_loop(0, 2 * per_half, step, 0)

    for b in UNITS:
        gate_up_unit(b)
    tokens.drain()
    chain.plane_forward(0)
    chain.plane_forward(1)

    ex.pass_on((2,))
    ex.finish((2,))
    samples.append(pltpu.make_async_copy(down_v.at[0], sample_down, loc_sem.at[3]))
    samples[-1].start()

    plane = fs % 4
    xp, yp = chain.xp, chain.yp
    xplane, yplane, dplane = chain.xplane, chain.yplane, 3 - plane
    mid, quarter = 3 * width // 8, 3 * width // 16
    tail, eighth = width // 4, width // 8
    last = pl.ds(2 * mid, tail)
    mixed = 2

    def columns(side):
        if side == mixed:
            return pl.ds(2 * mid, eighth), pl.ds(2 * mid + eighth, eighth)
        return pl.ds(side * mid, quarter), pl.ds(side * mid + quarter, quarter)

    def box_of(side):
        if side == mixed:
            return pl.ds(2 * quarter, eighth)
        return pl.ds(side * quarter, quarter)

    def number(b, side):
        return 8 if side == mixed else 2 * b + side

    def part(b, which, cols):
        return acts.at[b, pl.ds(which * share, share), cols]

    def down_unit(b, side):
        start = side * mid

        def step(n, carry):
            cols = pl.ds(pl.multiple_of(start + n * tile, tile), tile)
            acts[b, :, cols] = (
                dot_nt(hidden[b, :, 0:half], down_v[0, cols, :])
                + dot_nt(hidden[b, :, half : 2 * half], down_v[1, cols, :])
            ).astype(jnp.bfloat16)
            return carry

        lax.fori_loop(0, (tail if side == mixed else mid) // tile, step, 0)

    def d_copies(b, side):
        lo, hi = columns(side)
        box, n = box_of(side), number(b, side)
        return (
            remote(
                part(b, dplane, lo), xd_in.at[b, :, box], d_send.at[0, n], d_recv.at[0, n], xp, tp
            ),
            remote(
                part(b, dplane, hi), yd_in.at[b, :, box], d_send.at[1, n], d_recv.at[1, n], yp, tp
            ),
        )

    def g_copy(b, side, kind):
        lo, hi = columns(side)
        which, cols, box, to = (
            (xplane, lo, xg_in, xp),
            (xplane, hi, xg_in, xp),
            (yplane, hi, yg_in, yp),
            (yplane, lo, yg_in, yp),
        )[kind]
        n = number(b, side)
        return remote(
            part(b, which, cols), box.at[b, :, cols], g_send.at[kind, n], g_recv.at[kind, n],
            to, tp,
        )

    def first(b, side):
        for copy in d_copies(b, side):
            copy.start()
        g_copy(b, side, 0).start()
        g_copy(b, side, 2).start()

    def add_into(ref, others):
        total = ref[...].astype(jnp.float32)
        for other in others:
            total = total + other[...].astype(jnp.float32)
        ref[...] = total.astype(jnp.bfloat16)

    def combine(b, side):
        lo, hi = columns(side)
        box = box_of(side)
        x_copy, y_copy = d_copies(b, side)
        x_copy.wait_recv()
        add_into(part(b, yplane, lo), [xd_in.at[b, :, box]])
        g_copy(b, side, 3).start()
        y_copy.wait_recv()
        add_into(part(b, xplane, hi), [yd_in.at[b, :, box]])
        g_copy(b, side, 1).start()

    def z_box(b, way, cols):
        return (zb_in.at[max(b - 1, 0), :, cols], za_in.at[min(b, 2), :, cols])[way]

    def z_copy(b, side, way):
        cols = pl.ds(side * mid, mid)
        n = 2 * b + side
        return remote(
            part(b, plane, cols), z_box(b, way, cols), z_send.at[way, n], z_recv.at[way, n],
            fs + (4, -4)[way], tp,
        )

    def settle(b, side):
        cols = last if side == mixed else pl.ds(side * mid, mid)
        for kind in range(4):
            g_copy(b, side, kind).wait_recv()
        add_into(part(b, plane, cols), [xg_in.at[b, :, cols], yg_in.at[b, :, cols]])
        if side == mixed:
            return
        if b > 0:
            pl.when(z == 0)(z_copy(b, side, 0).start)
        if b < 3:
            pl.when(z == 3)(z_copy(b, side, 1).start)

    def relay(b, side, second):
        cols = pl.ds(side * mid, mid)
        for at, way in ((1, 0), (2, 0), (1, 1), (2, 1)):
            if (at >= b if way == 0 else at <= b):
                continue
            if second != ((way, at) in ((0, 2), (1, 1))):
                continue

            @pl.when(z == at)
            def _(way=way):
                z_copy(b, side, way).wait_recv()
                add_into(part(b, plane, cols), [z_box(b, way, cols)])
                z_copy(b, side, way).start()

    def finish(b):
        @pl.when(z == b)
        def _():
            for side in range(2):
                if b > 0:
                    z_copy(b, side, 0).wait_recv()
                if b < 3:
                    z_copy(b, side, 1).wait_recv()
            for side, lower, upper in ((0, 0, width // 2), (1, width // 2, 2 * mid)):
                cols = pl.ds(lower, upper - lower)
                total = acts[b, pl.ds(plane * share, share), cols].astype(jnp.float32)
                if b > 0:
                    total = total + z_box(b, 0, cols)[...].astype(jnp.float32)
                if b < 3:
                    total = total + z_box(b, 1, cols)[...].astype(jnp.float32)
                fin[side, :, 0 : upper - lower] = total.astype(jnp.bfloat16)
            fin[1, :, 2 * mid - width // 2 : width // 2] = acts[
                b, pl.ds(plane * share, share), last
            ]

    def l_box(b, way):
        return (lb_in.at[max(b - 1, 0)], la_in.at[min(b, 2)])[way]

    def line_copy(b, way):
        return remote(
            acts.at[b, :, last], l_box(b, way), l_send.at[way, b], l_recv.at[way, b],
            fs + (4, -4)[way], tp,
        )

    def line_start():
        for b in (3, 2, 1):
            pl.when(z == 0)(line_copy(b, 0).start)
        for b in (0, 1, 2):
            pl.when(z == 3)(line_copy(b, 1).start)

    def line_relay(b, at):
        way = 0 if at < b else 1

        @pl.when(z == at)
        def _():
            line_copy(b, way).wait_recv()
            add_into(acts.at[b, :, last], [l_box(b, way)])
            line_copy(b, way).start()

    def line_end(b):
        @pl.when(z == b)
        def _():
            boxes = []
            if b > 0:
                line_copy(b, 0).wait_recv()
                boxes.append(l_box(b, 0))
            if b < 3:
                line_copy(b, 1).wait_recv()
                boxes.append(l_box(b, 1))
            add_into(acts.at[b, :, last], boxes)

    puts = [
        pltpu.make_async_copy(common.at[:, pl.ds(i * half, half)], ref, loc_sem.at[4 + i])
        for i, ref in enumerate((common_gate, common_up, common_down))
    ]

    def shared_step(c, carry):
        a = normed[...]
        cols = pl.ds(pl.multiple_of(c * tile, tile), tile)
        gate = jnp.dot(a, common[:, cols], preferred_element_type=jnp.float32)
        up = jnp.dot(
            a, common[:, pl.ds(pl.multiple_of(half + c * tile, tile), tile)],
            preferred_element_type=jnp.float32,
        )
        shid[:, cols] = (jax.nn.silu(gate) * up).astype(jnp.bfloat16)
        return carry

    def shared_down_step(n, carry):
        per = width // 2 // tile
        spart[n // per, :, pl.ds(pl.multiple_of((n % per) * tile, tile), tile)] = dot_nt(
            shid[...],
            common[pl.ds(pl.multiple_of(n * tile, tile), tile), 2 * half : 3 * half],
        ).astype(jnp.bfloat16)
        return carry

    s_copy = remote(spart.at[1 - tp], spart_in, e_send.at[0], e_recv.at[0], fs, 1 - tp)

    def shared_expert():
        chain.finish()
        for copy in puts:
            copy.start()
        lax.fori_loop(0, per_half, shared_step, 0)
        lax.fori_loop(0, width // tile, shared_down_step, 0)
        s_copy.start()

    pieces = [(b, side) for b in UNITS for side in range(2)]
    count = len(pieces)
    for i in range(count + 6):
        if i < count:
            down_unit(*pieces[i])
            first(*pieces[i])
        if i == 0:
            for b in UNITS:
                down_unit(b, mixed)
            line_start()
        if i == 1:
            chain.plane_forward(2)
        if i == 2:
            chain.plane_forward(3)
        if i == 5:
            shared_expert()
        if 1 <= i <= count:
            combine(*pieces[i - 1])
        if 2 <= i <= count + 1:
            settle(*pieces[i - 2])
        if i == 2:
            line_relay(0, 2)
            line_relay(3, 1)
        if i == 3:
            line_relay(1, 2)
            line_relay(2, 1)
        if i == 4:
            line_relay(0, 1)
            line_relay(3, 2)
        if i == 6:
            for b in range(4):
                line_end(b)
            first(z, mixed)
        if i == 7:
            combine(z, mixed)
        if i == count + 1:
            settle(z, mixed)
        if 4 <= i < count + 4:
            relay(*pieces[i - 4], False)
        if i >= 6:
            relay(*pieces[i - 6], True)
    for b in UNITS:
        finish(b)
    f_copy = remote(fin.at[1 - tp], fin_in, e_send.at[1], e_recv.at[1], fs, 1 - tp)
    f_copy.start()
    s_copy.wait()
    near = pl.ds(pl.multiple_of(tp * share, share), share)
    far = pl.ds(pl.multiple_of((1 - tp) * share, share), share)
    f_copy.wait()
    for where, value in ((near, fin[tp]), (far, fin_in[...])):
        total = (
            spart[tp, where, :].astype(jnp.float32)
            + spart_in[where, :].astype(jnp.float32)
            + value.astype(jnp.float32)
        )
        out_ref[where, :] = total.astype(jnp.bfloat16)

    for copy in samples:
        copy.wait()
    for copy in puts:
        copy.wait()
    chain.drain()
    ex.drain()
    for b in range(4):
        if b > 0:
            pl.when(z < b)(line_copy(b, 0).wait_send)
        if b < 3:
            pl.when(z > b)(line_copy(b, 1).wait_send)
    for b, side in pieces + [(z, mixed)]:
        for copy in d_copies(b, side):
            copy.wait_send()
        for kind in range(4):
            g_copy(b, side, kind).wait_send()
        if side == mixed:
            continue
        if b > 0:
            pl.when(z < b)(z_copy(b, side, 0).wait_send)
        if b < 3:
            pl.when(z > b)(z_copy(b, side, 1).wait_send)


HBM = pl.BlockSpec(memory_space=pl.ANY)
VMEM = pl.BlockSpec(memory_space=pltpu.VMEM)
DMA = pltpu.SemaphoreType.DMA


def whole(tokens, scale, gain, shared, raw):
    experts, rows, half = raw[0].shape
    tok_rows, width = tokens.shape
    share = tok_rows // 2
    bf16, f32 = jnp.bfloat16, jnp.float32
    weight = jax.ShapeDtypeStruct((experts * rows, half), bf16)
    return pl.pallas_call(
        whole_kernel,
        out_shape=[jax.ShapeDtypeStruct((tok_rows, width // 2), bf16)] + [weight] * 6,
        in_specs=[HBM] + [VMEM] * 5 + [HBM] * 3,
        out_specs=[VMEM] + [HBM] * 6,
        scratch_shapes=[
            pltpu.VMEM((4, 4 * share, width), bf16),
            pltpu.VMEM((2, 2, width, half), bf16),
            pltpu.VMEM((2, width, half), bf16),
            pltpu.VMEM((experts, rows, half), f32),
            pltpu.VMEM((3, experts, rows, half), bf16),
            pltpu.VMEM((4, 4 * share, 2 * half), bf16),
            pltpu.VMEM((width, 3 * half), bf16),
            pltpu.VMEM((tok_rows, width), bf16),
            pltpu.VMEM((experts, 1, share), f32),
            pltpu.VMEM((experts * share, 1), f32),
            pltpu.VMEM((tok_rows, half), bf16),
            pltpu.VMEM((2, tok_rows, width // 2), bf16),
            pltpu.VMEM((tok_rows, width // 2), bf16),
            pltpu.VMEM((2, share, width // 2), bf16),
            pltpu.VMEM((share, width // 2), bf16),
            pltpu.VMEM((4, share, width // 2), bf16),
            pltpu.VMEM((4, share, width // 2), bf16),
            pltpu.VMEM((4, share, width), bf16),
            pltpu.VMEM((4, share, width), bf16),
            pltpu.VMEM((3, share, 3 * width // 4), bf16),
            pltpu.VMEM((3, share, 3 * width // 4), bf16),
            pltpu.VMEM((3, 4 * share, width // 4), bf16),
            pltpu.VMEM((3, 4 * share, width // 4), bf16),
            DMA((4, 4)), DMA((4,)), DMA((16,)), DMA((4, 4)), DMA((4,)), DMA((16,)),
            DMA((16,)), DMA((16,)),
            DMA((3, 16)), DMA((3, 16)), DMA((3, 16)), DMA((3, 16)), DMA((3, 16)),
            DMA((2, 9)), DMA((2, 9)), DMA((4, 9)), DMA((4, 9)), DMA((2, 8)), DMA((2, 8)),
            DMA((2, 4)), DMA((2, 4)),
            DMA((2,)), DMA((2,)), DMA((8,)),
        ],
        compiler_params=pltpu.CompilerParams(
            collective_id=1, has_side_effects=True, vmem_limit_bytes=67043328
        ),
        name="whole",
    )(tokens, scale, gain, *shared, *raw)


def emit_kernel(count, *refs):
    source, target, boxes = refs[:count], refs[count : 2 * count], refs[2 * count : -2]
    in_sem, out_sem = refs[-2:]
    parts = []
    for i in range(count):
        length = source[i].shape[0] // 4
        for c in range(4):
            at = pl.ds(c * length, length)
            parts.append((
                pltpu.make_async_copy(source[i].at[at], boxes[i].at[at], in_sem.at[i, c]),
                pltpu.make_async_copy(boxes[i].at[at], target[i].at[at], out_sem.at[i, c]),
            ))
    for load, _ in parts:
        load.start()
    for load, store in parts:
        load.wait()
        store.start()
    for _, store in parts:
        store.wait()


def emit(*arrays):
    n = len(arrays)
    shapes = [jax.ShapeDtypeStruct(a.shape, a.dtype) for a in arrays]
    return pl.pallas_call(
        functools.partial(emit_kernel, n),
        out_shape=shapes,
        in_specs=[HBM] * n,
        out_specs=[HBM] * n,
        scratch_shapes=[pltpu.VMEM(a.shape, a.dtype) for a in arrays]
        + [DMA((n, 4)), DMA((n, 4))],
        compiler_params=pltpu.CompilerParams(vmem_limit_bytes=67043328),
        name="emit",
    )(*arrays)


def ring_of(fs_count):
    if fs_count != 16:
        return list(range(fs_count))
    order = []
    for place, column in enumerate((0, 1, 3, 2)):
        heights = range(4) if place % 2 == 0 else range(3, -1, -1)
        order.extend(height * 4 + column for height in heights)
    return order


def reorder(blocks, order):
    if list(order) == list(range(len(order))):
        return blocks
    return jnp.concatenate([blocks[i : i + 1] for i in order], axis=0)


def general_body(
    tokens,
    routes,
    route_weights,
    norm_gain,
    expert_gate,
    expert_up,
    expert_down,
    shared_gate,
    shared_up,
    shared_down,
):
    tp_count = lax.axis_size("tp")
    tp_index = lax.axis_index("tp")
    fs_count = lax.axis_size("fs")
    tok_rows, width = tokens.shape
    experts = expert_gate.shape[0]
    share = tok_rows // tp_count
    own_experts = experts // fs_count
    ring = ring_of(fs_count)
    place_of = [ring.index(i) for i in range(fs_count)]
    groups = None if ring == list(range(fs_count)) else [ring]

    normed = normalize(tokens)
    own_normed = lax.dynamic_slice_in_dim(normed, tp_index * share, share, 0)
    own_routes = lax.dynamic_slice_in_dim(routes, tp_index * share, share, 0)
    own_weights = lax.dynamic_slice_in_dim(route_weights, tp_index * share, share, 0)
    member = own_routes[None, :, :] == jnp.arange(experts, dtype=jnp.int32)[:, None, None]
    dense = jnp.sum(jnp.where(member, own_weights[None, :, :], 0.0), axis=2)
    dense_all = lax.all_gather(dense, "fs", axis=0, tiled=False)
    own_normed, dense_all = lax.optimization_barrier((own_normed, dense_all))
    gathered = lax.all_gather(own_normed, "fs", axis=0, tiled=False)
    gathered = reorder(gathered, ring).reshape(fs_count * share, width)

    gain_rows = norm_gain[None, :, None]
    rounded = (
        (expert_gate * gain_rows).astype(jnp.bfloat16),
        (expert_up * gain_rows).astype(jnp.bfloat16),
        expert_down.astype(jnp.bfloat16),
    )
    sample_gate, sample_up, sample_down = (
        lax.all_to_all(rounded[0], "fs", split_axis=0, concat_axis=1, tiled=True),
        lax.all_to_all(rounded[1], "fs", split_axis=0, concat_axis=1, tiled=True),
        lax.all_to_all(rounded[2], "fs", split_axis=0, concat_axis=1, tiled=True),
    )

    half = shared_gate.shape[1]
    shared_rows = jnp.concatenate(
        [
            (shared_gate * norm_gain[:, None]).astype(jnp.bfloat16),
            (shared_up * norm_gain[:, None]).astype(jnp.bfloat16),
            shared_down.astype(jnp.bfloat16),
        ],
        axis=1,
    )
    common = lax.all_gather(shared_rows, "fs", axis=0, tiled=False, axis_index_groups=groups)
    common_gate, common_up, common_down = (
        reorder(common[:, :, i * half : (i + 1) * half], place_of).reshape(width, half)
        for i in range(3)
    )
    shared_gate_act = jnp.dot(normed, common_gate, preferred_element_type=jnp.float32)
    shared_up_act = jnp.dot(normed, common_up, preferred_element_type=jnp.float32)
    shared_hidden = (jax.nn.silu(shared_gate_act) * shared_up_act).astype(jnp.bfloat16)
    shared_part = jnp.einsum(
        "th,dh->td", shared_hidden, common_down, preferred_element_type=jnp.float32
    ).astype(jnp.bfloat16)
    shared_parts = lax.all_to_all(
        shared_part.reshape(tok_rows, tp_count, width // tp_count).transpose(1, 0, 2),
        "tp",
        split_axis=0,
        concat_axis=0,
        tiled=True,
    )
    shared_sum = jnp.sum(shared_parts.astype(jnp.float32), axis=0)

    scale_all = reorder(
        lax.dynamic_slice_in_dim(
            dense_all, lax.axis_index("fs") * own_experts, own_experts, 1
        ),
        ring,
    )
    total = None
    for expert in range(own_experts):
        scale = scale_all[:, expert, :].reshape(-1)[:, None]
        for shift in range(tp_count):
            gate_w, up_w, down_w = (
                sample_gate[expert],
                sample_up[expert],
                sample_down[expert],
            )
            if shift:
                pairs = [(i, (i + shift) % tp_count) for i in range(tp_count)]
                gate_w, up_w, down_w = (
                    lax.ppermute(gate_w, "tp", pairs),
                    lax.ppermute(up_w, "tp", pairs),
                    lax.ppermute(down_w, "tp", pairs),
                )
            gate = jnp.dot(gathered, gate_w, preferred_element_type=jnp.float32)
            upward = jnp.dot(gathered, up_w, preferred_element_type=jnp.float32)
            hidden = (jax.nn.silu(gate) * upward * scale).astype(jnp.bfloat16)
            part = jnp.einsum("rf,df->rd", hidden, down_w, preferred_element_type=jnp.float32)
            total = part if total is None else total + part
    routed = lax.psum_scatter(
        total.astype(jnp.bfloat16), "fs", scatter_dimension=0, tiled=True, axis_index_groups=groups
    )
    routed = lax.all_to_all(routed, "tp", split_axis=1, concat_axis=0, tiled=True)
    layer_output = (routed.astype(jnp.float32) + shared_sum).astype(jnp.bfloat16)
    return (layer_output, sample_gate, sample_up, sample_down, common_gate, common_up, common_down)

def block_body(
    tokens, routes, route_weights, norm_gain,
    expert_gate, expert_up, expert_down,
    shared_gate, shared_up, shared_down,
):
    tok_rows = tokens.shape[0]
    experts = expert_gate.shape[0]
    share = tok_rows // 2
    member = routes[None, :, :] == jnp.arange(experts, dtype=jnp.int32)[:, None, None]
    dense = jnp.sum(jnp.where(member, route_weights[None, :, :], 0.0), axis=2)
    gain = norm_gain[None, :]
    outputs = whole(
        tokens, dense.reshape(experts, 2, 1, share), gain,
        (shared_gate, shared_up, shared_down), (expert_gate, expert_up, expert_down),
    )
    (
        layer_output, sample_gate, sample_up, sample_down, common_gate, common_up, common_down
    ) = emit(*outputs)
    return (
        layer_output, sample_gate[None], sample_up[None], sample_down[None],
        common_gate, common_up, common_down,
    )


def solution(mesh):
    fits = mesh.shape["fs"] == 16 and mesh.shape["tp"] == 2
    body = block_body if fits else general_body
    return jax.shard_map(
        body,
        mesh=mesh,
        in_specs=(
            P("fs", None),
            P("fs", None),
            P("fs", None),
            P("fs"),
            P(None, "fs", "tp"),
            P(None, "fs", "tp"),
            P(None, "fs", "tp"),
            P("fs", "tp"),
            P("fs", "tp"),
            P("fs", "tp"),
        ),
        out_specs=(
            P("fs", "tp"),
            P("fs", None, "tp"),
            P("fs", None, "tp"),
            P("fs", None, "tp"),
            P(None, "tp"),
            P(None, "tp"),
            P(None, "tp"),
        ),
        check_vma=False,
    )
```
